256 devices in a mesh: ep: 32 (over z, x), tp: 8 (over y, core).
Axes of the slice: x: 4, y: 4, z: 8, core: 2. Of those that a mesh axis runs over, the one named last changes fastest.
Arguments:
- tokens: bfloat16 [2048, 2048], P('ep', 'tp')
- norm_gain: float32 [2048], P('tp'), may hold values from 0.1 to 1.9
- expert_ids: int32 [2048, 4], P('ep'), may hold values from 0 to 31, all different within a row; in each aligned block of 64 rows (0 to 63, 64 to 127, ...) at most 16 rows name the same one
- route_weights: float32 [2048, 4], P('ep'), may hold values from 0.1 to 1
- gate_proj: bfloat16 [32, 2048, 2048], P('ep', None, 'tp'), may hold values from -0.5 to 0.5
- up_proj: bfloat16 [32, 2048, 2048], P('ep', None, 'tp'), may hold values from -0.5 to 0.5
- down_proj: bfloat16 [32, 2048, 2048], P('ep', 'tp')
- final_gain: float32 [2048], P('tp'), may hold values from 0.1 to 1.9
Outputs:
- layer_output: bfloat16 [2048, 2048], P('ep', 'tp')
The draws below stay inside these ranges and needn't reach their ends.
Inputs may be any that keep to these rules, and one draw needn't show every extreme that they name: `expert_ids`: each row names 4 different experts. Within the 64 rows of one device no expert is named by more than 16 rows, a bound that some block reaches.
All inputs are finite; a program needn't handle non-finite values.
Results may differ from the reference program's by a relative error of at most 0.017.
Values may be sent and summed in bfloat16 or wider, within the bound.
A program may use at most 64 MiB of HBM per device.

```python
import math
import jax
import jax.numpy as jnp
import numpy as np
from jax import lax

D = 2048
FF = 2048
TOP_K = 4
TOK_DEV = 64
EXPERTS = 32
TOKENS = 2048
CAP = 16
N_EP = 32
N_TP = 8


def column_rise(count):
    return jnp.exp(math.log(6.0) * jnp.arange(count, dtype=jnp.float32) / (count - 1))


def draw_tokens(key, part):
    first_key, second_key = jax.random.split(key, 2)
    row_scales = jnp.exp(jax.random.uniform(second_key, (TOKENS, 1), jnp.float32, minval=math.log(0.3), maxval=math.log(3.0)))
    base = jax.random.normal(first_key, (TOKENS, D), jnp.float32)
    return (base * row_scales * column_rise(D)[None, :]).astype(jnp.bfloat16)


def draw_down_proj(key, part):
    first_key = jax.random.fold_in(key, 0)
    base = jax.random.normal(first_key, (EXPERTS, FF, D), jnp.float32)
    return (base * FF ** (-0.5) * column_rise(D)[None, None, :]).astype(jnp.bfloat16)


def shard_levels(key, extent, shards, low, top_value):
    def one(axis_at, blocks):
        steps = jax.random.uniform(jax.random.fold_in(jax.random.fold_in(key, 6), axis_at), (blocks,), jnp.float32, low / len(shards), top_value / len(shards))
        return jnp.repeat(jnp.exp(steps), extent[axis_at] // blocks).reshape((-1,) + (1,) * (len(extent) - axis_at - 1))

    gain = one(*shards[0])
    for cut in shards[1:]:
        gain = gain * one(*cut)
    return gain


def assign_block(own_key, own, number, rows, amount, top, most, skew):
    ranking = jax.random.permutation(own_key, amount)
    packed, ordinary = portions_of(amount, rows * top, most, skew, True), portions_of(amount, rows * top, most, skew, False)
    places = jnp.arange(amount)

    def named(lengths, turn):
        used = int((lengths > 0).sum())
        fixed = max(1, used // 4)
        moved = fixed + (places - fixed + turn * (used - fixed)) % max(1, amount - fixed)
        return jnp.zeros((amount,), jnp.int32).at[ranking[jnp.where(places < fixed, places, moved)]].set(jnp.asarray(lengths, jnp.int32))

    lengths = jnp.where(number % 4 == 0, named(packed, number // 4), named(ordinary, number - number // 4 - 1))
    mixed = jax.random.permutation(jax.random.fold_in(own, 3), amount)
    giver, sink = mixed[0:amount // 2 * 2:2], mixed[1:amount // 2 * 2:2]
    margin = jnp.minimum(lengths[giver] - 1, most - lengths[sink]) // 2
    margin = jnp.where((giver == ranking[0]) | (sink == ranking[0]) | (lengths[sink] == 0), 0, jnp.maximum(margin, 0))
    moved = jax.random.randint(jax.random.fold_in(own, 4), (amount // 2,), 0, 1 << 20) % (margin + 1)
    lengths = lengths.at[giver].add(-moved).at[sink].add(moved)
    labels = jnp.searchsorted(jnp.cumsum(lengths), jnp.arange(rows * top), side="right").astype(jnp.int32)
    table = labels.reshape(top, rows).T
    table = table[jax.random.permutation(jax.random.fold_in(own, 1), rows)]
    turn = jax.random.randint(jax.random.fold_in(own, 2), (rows, 1), 0, top)
    return jnp.take_along_axis(table, (jnp.arange(top)[None, :] + turn) % top, axis=1)


def portions_of(number_of, total, limit, skew, full):
    portions = [(1 << 20) // math.isqrt(rank ** skew) + 1 for rank in range(1, number_of + 1)]
    largest = limit if full else min(limit, max(-(-total // number_of), total * portions[0] // sum(portions)))
    least = 1 if total - largest >= number_of - 1 else 0
    counts, spare = [largest] + [least] * (number_of - 1), total - largest - least * (number_of - 1)
    while spare > 0:
        candidates = [i for i in range(1, number_of) if counts[i] < largest] or [i for i in range(1, number_of) if counts[i] < limit]
        pool, budget = sum([portions[i] for i in candidates]), spare
        for i in candidates:
            more = min(limit - counts[i], max(1, budget * portions[i] // pool), spare)
            counts[i] = counts[i] + more
            spare = spare - more
    return np.array(counts)


def normal_values(own_key, shape, scale, limit, cuts=(), kind=jnp.bfloat16):
    result = scale * jax.random.normal(own_key, shape, jnp.float32)
    if cuts:
        result = result * shard_levels(own_key, shape, cuts, -0.22, 0.18)
    return jnp.clip(result, -limit, limit).astype(kind)


def setup_inputs(seed: int = 0) -> dict:
    splits = jax.random.split(jax.random.key(seed), 9)
    tokens = draw_tokens(jax.random.fold_in(splits[8], 71), 0)
    norm_gain = jnp.clip(1.0 + 0.18 * jax.random.normal(splits[1], (D,), jnp.float32), 0.1, 1.9)
    expert_ids_keys = jax.random.split(jax.random.fold_in(splits[2], 1), TOKENS // TOK_DEV)
    expert_ids_turns = jax.random.permutation(jax.random.fold_in(splits[2], 3), TOKENS // TOK_DEV)
    expert_ids = jax.vmap(lambda own, number: assign_block(jax.random.fold_in(splits[2], 2), own, number, TOK_DEV, EXPERTS, TOP_K, CAP, 2))(expert_ids_keys, expert_ids_turns).reshape((TOKENS, TOP_K))
    route_weights = jnp.clip(0.1 + 0.9 * jax.random.uniform(splits[3], (TOKENS, TOP_K), jnp.float32) ** shard_levels(splits[3], (TOKENS, TOP_K), ((0, 32),), -0.2, 0.2), 0.1, 1.0)
    gate_proj = normal_values(splits[4], (EXPERTS, D, FF), (D // 16) ** -0.5, 0.5, ((0, 32), (2, 8)))
    up_proj = normal_values(splits[5], (EXPERTS, D, FF), (D // 16) ** -0.5, 0.5, ((0, 32), (2, 8)))
    down_proj = draw_down_proj(jax.random.fold_in(splits[8], 71), 0)
    final_gain = jnp.clip(1.0 + 0.18 * jax.random.normal(splits[7], (D,), jnp.float32), 0.1, 1.9)
    return {"tokens": tokens, "norm_gain": norm_gain, "expert_ids": expert_ids, "route_weights": route_weights, "gate_proj": gate_proj, "up_proj": up_proj, "down_proj": down_proj, "final_gain": final_gain}


EPSILON = 1e-05
CLAMP_LIMIT = 7.0
SIGMOID_SLOPE = 1.702

def slot_tables(id_block, gate_block, targets, capacity):
    matches = (id_block[:, :, None] == targets[None, None, :]).astype(jnp.int32)
    per_token = lax.optimization_barrier(jnp.sum(matches, axis=1))
    earlier = jnp.cumsum(per_token, axis=0) - per_token
    slot_places = lax.broadcasted_iota(jnp.int32, (1, 1, capacity), 2)
    selector = (per_token[:, :, None] * (earlier[:, :, None] == slot_places).astype(jnp.int32)).astype(jnp.float32)
    weights = lax.optimization_barrier(jnp.sum(gate_block[:, :, None] * matches.astype(jnp.float32), axis=1))
    return (selector, weights)

def reference(tokens, norm_gain, expert_ids, route_weights, gate_proj, up_proj, down_proj, final_gain):
    input_rows = tokens.astype(jnp.float32)
    row_scale = lax.rsqrt(lax.optimization_barrier(jnp.mean(input_rows * input_rows, axis=1, keepdims=True)) + EPSILON)
    normed = (input_rows * row_scale * norm_gain[None, :]).astype(jnp.bfloat16)
    targets = jnp.arange(EXPERTS, dtype=jnp.int32)

    def per_source(id_block, gate_block):
        return slot_tables(id_block, gate_block, targets, CAP)
    selector, weights = jax.vmap(per_source)(expert_ids.reshape(N_EP, TOK_DEV, TOP_K), route_weights.reshape(N_EP, TOK_DEV, TOP_K))
    blocks = normed.reshape(N_EP, TOK_DEV, D).astype(jnp.float32)
    select_by_expert = jnp.moveaxis(selector, 2, 0)
    weight_by_expert = jnp.moveaxis(weights, 2, 0)

    def one_expert(carry, inputs):
        chosen, gate_share, gate_w, up_w, down_w = inputs
        expert_rows = jnp.einsum('stc,std->scd', chosen, blocks).astype(jnp.bfloat16).reshape(-1, D)
        gate_pre = jnp.minimum(jnp.dot(expert_rows, gate_w, preferred_element_type=jnp.float32), CLAMP_LIMIT)
        up_pre = jnp.clip(jnp.dot(expert_rows, up_w, preferred_element_type=jnp.float32), -CLAMP_LIMIT, CLAMP_LIMIT)
        activated = ((up_pre + 1.0) * gate_pre * jax.nn.sigmoid(SIGMOID_SLOPE * gate_pre)).astype(jnp.bfloat16)
        partials = jnp.einsum('npf,pfd->npd', activated.reshape(-1, N_TP, FF // N_TP).astype(jnp.float32), down_w.reshape(N_TP, FF // N_TP, D).astype(jnp.float32))
        rounded = lax.optimization_barrier(partials.astype(jnp.bfloat16))
        expert_out = lax.optimization_barrier(jnp.sum(rounded.astype(jnp.float32), axis=1)).astype(jnp.bfloat16)
        contrib = jnp.einsum('stc,scd->std', chosen * gate_share[:, :, None], expert_out.astype(jnp.float32).reshape(N_EP, CAP, D))
        return (carry + contrib, None)
    summed, _ = lax.scan(one_expert, jnp.zeros((N_EP, TOK_DEV, D), jnp.float32), (select_by_expert, weight_by_expert, gate_proj, up_proj, down_proj))
    mixture = summed.reshape(TOKENS, D)
    out_scale = lax.rsqrt(lax.optimization_barrier(jnp.mean(mixture * mixture, axis=1, keepdims=True)) + EPSILON)
    return (mixture * out_scale * final_gain[None, :]).astype(jnp.bfloat16)
```

```python
import functools

import jax
import jax.numpy as jnp
from jax import lax
from jax.experimental import pallas as pl
from jax.experimental.pallas import tpu as pltpu
from jax.sharding import PartitionSpec as P

MESH = pl.DeviceIdType.MESH
EPSILON = 1e-05
CLAMP_LIMIT = 7.0
SIGMOID_SLOPE = 1.702
F32 = jnp.float32
BF16 = jnp.bfloat16
HIGHEST = lax.Precision.HIGHEST

NZ, NX, NY = 8, 4, 4
N_EP, N_TP = NZ * NX, NY * 2
TOK, CAP, W = 64, 16, 256
D = N_TP * W
K = 4
R = N_EP * CAP // K
PER = N_EP // K


def z_offset(i):
    h = (i + 1) // 2
    return h if i % 2 else (NZ - h) % NZ


def remote(src, dst, send_sem, recv_sem, ep, tp):
    return pltpu.make_async_remote_copy(
        src_ref=src, dst_ref=dst, send_sem=send_sem, recv_sem=recv_sem, device_id=(ep, tp), device_id_type=MESH
    )


def dot(a, b, dims=((1,), (0,)), precision=None):
    return lax.dot_general(a, b, (dims, ((), ())), precision=precision, preferred_element_type=F32)


def kernel(
    tok, ngain, ids, rw, wg_h, wu_h, wd_h, fgain, out,
    wg, wu, wd, gbuf, sbuf, xbuf, ps, q, po, ts, ra, rb, rc, obuf, ybuf, fbuf, wsel,
    wsem, bulk, gsem, a_recv, ag_send, ag_recv, rs_send, rs_recv, y_recv, f_recv,
):
    me_ep, me_tp = lax.axis_index("ep"), lax.axis_index("tp")
    z, x = me_ep // NX, lax.rem(me_ep, NX)
    y, c = me_tp // 2, lax.rem(me_tp, 2)
    d = 1 - 2 * c
    co = 1 - c
    yp, ym, yf = lax.rem(y + d + NY, NY), lax.rem(y - d + NY, NY), lax.rem(y + 2, NY)

    def at(yy, cc):
        return yy * 2 + cc

    def back(p):
        return lax.rem(z - z_offset(p // NX) + NZ, NZ) * NX + lax.rem(x - p % NX + NX, NX)

    def forth(p):
        return lax.rem(z + z_offset(p // NX), NZ) * NX + lax.rem(x + p % NX, NX)

    def peer(i):
        return lax.rem(me_tp + i, N_TP)

    barrier = pltpu.get_barrier_semaphore()
    for p in range(1, N_EP):
        pl.semaphore_signal(barrier, inc=1, device_id=(back(p), me_tp), device_id_type=MESH)
    for i in range(1, N_TP):
        pl.semaphore_signal(barrier, inc=1, device_id=(me_ep, peer(i)), device_id_type=MESH)

    loads = [
        pltpu.make_async_copy(wg_h.at[0], wg, wsem.at[0]),
        pltpu.make_async_copy(wu_h.at[0], wu, wsem.at[1]),
        pltpu.make_async_copy(wd_h.at[0], wd, wsem.at[2]),
    ]
    for load in loads:
        load.start()

    pos = lax.broadcasted_iota(jnp.int32, (TOK, N_EP), 1)
    zi, dx = pos // NX, lax.rem(pos, NX)
    half = (zi + 1) // 2
    dz = jnp.where(lax.rem(zi, 2) == 1, half, NZ - half)
    expert = lax.rem(z - dz + 2 * NZ, NZ) * NX + lax.rem(x - dx + NX, NX)
    match = jnp.zeros((TOK, N_EP), F32)
    weight = jnp.zeros((TOK, N_EP), F32)
    for k in range(ids.shape[1]):
        hit = ids[:, k : k + 1] == expert
        match = match + jnp.where(hit, 1.0, 0.0)
        weight = weight + jnp.where(hit, rw[:, k : k + 1], 0.0)
    before = lax.broadcasted_iota(jnp.int32, (TOK, TOK), 0) > lax.broadcasted_iota(jnp.int32, (TOK, TOK), 1)
    earlier = dot(jnp.where(before, 1.0, 0.0).astype(BF16), match.astype(BF16))
    col = lax.broadcasted_iota(jnp.int32, (N_EP, N_EP * CAP), 1)
    row = lax.broadcasted_iota(jnp.int32, (N_EP, N_EP * CAP), 0)
    spread = jnp.where(col // CAP == row, 1.0, 0.0).astype(BF16)
    slot = lax.rem(lax.broadcasted_iota(jnp.int32, (TOK, N_EP * CAP), 1), CAP).astype(F32)
    taken = (dot(earlier.astype(BF16), spread) == slot) & (dot(match.astype(BF16), spread) > 0.5)
    w_hi = weight.astype(BF16)
    w_lo = (weight - w_hi.astype(F32)).astype(BF16)
    wide = dot(w_hi, spread) + dot(w_lo, spread)
    wsel[...] = jnp.where(taken, wide, 0.0)
    rows = dot(jnp.where(taken, 1.0, 0.0).astype(BF16), tok[...], ((0,), (0,))).astype(BF16)
    sbuf[...] = rows
    xbuf[me_tp, 0:CAP] = rows[0:CAP]
    gbuf[me_tp] = jnp.broadcast_to(ngain[...].reshape(1, W), (8, W))
    pl.semaphore_wait(barrier, N_EP - 1 + N_TP - 1)

    def block(p):
        return pl.ds(p * CAP, CAP)

    def chunk(k):
        return pl.ds(k * R, R)

    for p in range(1, N_EP):
        remote(sbuf.at[block(p)], xbuf.at[me_tp, block(p)], bulk.at[0], a_recv.at[p // PER], back(p), me_tp).start()
    gains = [remote(gbuf.at[me_tp], gbuf.at[me_tp], gsem.at[0, i - 1], gsem.at[1, i - 1], me_ep, peer(i)) for i in range(1, N_TP)]
    for copy in gains:
        copy.start()
    sends = list(gains)

    def send(src, dst, send_sem, recv_sem, tp):
        copy = remote(src, dst, send_sem, recv_sem, me_ep, tp)
        copy.start()
        sends.append(copy)

    def arrived(ref, sem):
        remote(ref, ref, bulk.at[0], sem, me_ep, at(yp, c)).wait_recv()

    def gather_own(k):
        ref = xbuf.at[me_tp, pl.ds(CAP, R - CAP)] if k == 0 else xbuf.at[me_tp, chunk(k)]
        arrived(ref, a_recv.at[k])
        ref = xbuf.at[me_tp, chunk(k)]
        send(ref, ref, ag_send.at[k, 0], ag_recv.at[k, 0], at(yp, c))
        send(ref, ref, ag_send.at[k, 1], ag_recv.at[k, 1], at(ym, c))
        send(ref, ref, ag_send.at[k, 2], ag_recv.at[k, 2], at(y, co))

    def gather_near(k):
        ref = xbuf.at[at(ym, c), chunk(k)]
        arrived(ref, ag_recv.at[k, 0])
        send(ref, ref, ag_send.at[k, 3], ag_recv.at[k, 3], at(yp, c))
        send(ref, ref, ag_send.at[k, 4], ag_recv.at[k, 4], at(y, co))
        ref = xbuf.at[at(yp, c), chunk(k)]
        arrived(ref, ag_recv.at[k, 1])
        send(ref, ref, ag_send.at[k, 5], ag_recv.at[k, 5], at(y, co))

    def gather_far(k):
        ref = xbuf.at[at(yf, c), chunk(k)]
        arrived(ref, ag_recv.at[k, 3])
        send(ref, ref, ag_send.at[k, 6], ag_recv.at[k, 6], at(y, co))

    def compute(k):
        if k == 0:
            for load in loads:
                load.wait()
            for copy in gains:
                copy.wait_recv()
        arrived(xbuf.at[at(y, co), chunk(k)], ag_recv.at[k, 2])
        arrived(xbuf.at[at(yp, co), chunk(k)], ag_recv.at[k, 4])
        arrived(xbuf.at[at(ym, co), chunk(k)], ag_recv.at[k, 5])
        arrived(xbuf.at[at(yf, co), chunk(k)], ag_recv.at[k, 6])
        squares = jnp.zeros((R, W), F32)
        for t in range(N_TP):
            part = xbuf[t, chunk(k)].astype(F32)
            squares = squares + part * part
        scale = lax.rsqrt(jnp.sum(squares, axis=1, keepdims=True) / D + EPSILON)
        gate = jnp.zeros((R, W), F32)
        up = jnp.zeros((R, W), F32)
        for t in range(N_TP):
            part = xbuf[t, chunk(k)].astype(F32)
            normed = (part * scale * gbuf[t, 0:1, :]).astype(BF16)
            gate = gate + dot(normed, wg[t * W : (t + 1) * W, :])
            up = up + dot(normed, wu[t * W : (t + 1) * W, :])
        gate = jnp.minimum(gate, CLAMP_LIMIT)
        up = jnp.clip(up, -CLAMP_LIMIT, CLAMP_LIMIT)
        act = ((up + 1.0) * gate * jax.nn.sigmoid(SIGMOID_SLOPE * gate)).astype(BF16)
        for r in range(NY):
            theirs = at(lax.rem(y - r * d + 2 * NY, NY), co)
            ps[k, r] = dot(act, wd[:, pl.ds(pl.multiple_of(theirs * W, W), W)]).astype(BF16)
        send(ps.at[k], q.at[k], rs_send.at[k, 0], rs_recv.at[k, 0], at(y, co))
        for r in range(NY):
            mine = at(lax.rem(y + r * d + 2 * NY, NY), c)
            po[k, r] = dot(act, wd[:, pl.ds(pl.multiple_of(mine * W, W), W)])

    def pair_sum(k):
        arrived(q.at[k], rs_recv.at[k, 0])
        ts[k, 0] = (po[k, 2] + q[k, 2].astype(F32)).astype(BF16)
        send(ts.at[k, 0], ra.at[k], rs_send.at[k, 1], rs_recv.at[k, 1], at(yp, c))
        ts[k, 1] = (po[k, 3] + q[k, 3].astype(F32)).astype(BF16)
        send(ts.at[k, 1], rb.at[k], rs_send.at[k, 2], rs_recv.at[k, 2], at(ym, c))

    def chain(k):
        arrived(ra.at[k], rs_recv.at[k, 1])
        ts[k, 2] = (po[k, 1] + q[k, 1].astype(F32) + ra[k].astype(F32)).astype(BF16)
        send(ts.at[k, 2], rc.at[k], rs_send.at[k, 3], rs_recv.at[k, 3], at(yp, c))

    def finish(k):
        arrived(rb.at[k], rs_recv.at[k, 2])
        arrived(rc.at[k], rs_recv.at[k, 3])
        total = po[k, 0] + q[k, 0].astype(F32) + rb[k].astype(F32) + rc[k].astype(F32)
        obuf[chunk(k)] = total.astype(BF16)
        if k == 0:
            ybuf[0:CAP] = total[0:CAP].astype(BF16)
        for p in range(max(1, k * PER), (k + 1) * PER):
            remote(obuf.at[block(p)], ybuf.at[block(p)], bulk.at[1], y_recv.at[k], forth(p), me_tp).start()

    stages = [gather_own, gather_near, gather_far, compute, pair_sum, chain, finish]
    for step in range(K + len(stages) - 1):
        for s in reversed(range(len(stages))):
            if 0 <= step - s < K:
                stages[s](step - s)

    mixture = jnp.zeros((TOK, W), F32)
    for k in range(K):
        arrived(ybuf.at[pl.ds(CAP, R - CAP)] if k == 0 else ybuf.at[chunk(k)], y_recv.at[k])
        part = wsel[:, k * R : (k + 1) * R]
        hi = part.astype(BF16)
        lo = (part - hi.astype(F32)).astype(BF16)
        values = ybuf[chunk(k)]
        mixture = mixture + dot(hi, values) + dot(lo, values)
    ones = jnp.ones((8, W), F32)
    sums = dot(ones, mixture * mixture, ((1,), (1,)), HIGHEST)
    fbuf[me_tp] = jnp.concatenate([sums, jnp.zeros((8, 128 - TOK), F32)], axis=1)
    finals = [remote(fbuf.at[me_tp], fbuf.at[me_tp], f_recv.at[0, i - 1], f_recv.at[1, i - 1], me_ep, peer(i)) for i in range(1, N_TP)]
    for copy in finals:
        copy.start()
    for copy in finals:
        copy.wait_recv()
    total = jnp.zeros((8, 128), F32)
    for t in range(N_TP):
        total = total + fbuf[t]
    scale = lax.rsqrt(total / D + EPSILON)
    first = jnp.where(lax.broadcasted_iota(jnp.int32, (8, W), 0) == 0, 1.0, 0.0)
    tall = dot(scale, first, ((0,), (0,)), HIGHEST)[:TOK]
    out[...] = (mixture * tall * fgain[...].reshape(1, W)).astype(BF16)

    for copy in sends + finals:
        copy.wait_send()
    remote(sbuf.at[pl.ds(CAP, N_EP * CAP - CAP)], sbuf.at[pl.ds(CAP, N_EP * CAP - CAP)], bulk.at[0], bulk.at[0], me_ep, at(yp, c)).wait_send()
    remote(obuf.at[pl.ds(CAP, N_EP * CAP - CAP)], obuf.at[pl.ds(CAP, N_EP * CAP - CAP)], bulk.at[1], bulk.at[1], me_ep, at(yp, c)).wait_send()


def step(tokens, norm_gain, expert_ids, route_weights, gate_proj, up_proj, down_proj, final_gain):
    vmem = pl.BlockSpec(memory_space=pltpu.VMEM)
    hbm = pl.BlockSpec(memory_space=pl.ANY)
    rows = N_EP * CAP
    dma = pltpu.SemaphoreType.DMA
    return pl.pallas_call(
        kernel,
        out_shape=jax.ShapeDtypeStruct((TOK, W), BF16),
        in_specs=[vmem, vmem, vmem, vmem, hbm, hbm, hbm, vmem],
        out_specs=vmem,
        scratch_shapes=[
            pltpu.VMEM((D, W), BF16),
            pltpu.VMEM((D, W), BF16),
            pltpu.VMEM((W, D), BF16),
            pltpu.VMEM((N_TP, 8, W), F32),
            pltpu.VMEM((rows, W), BF16),
            pltpu.VMEM((N_TP, rows, W), BF16),
            pltpu.VMEM((K, NY, R, W), BF16),
            pltpu.VMEM((K, NY, R, W), BF16),
            pltpu.VMEM((K, NY, R, W), F32),
            pltpu.VMEM((K, 3, R, W), BF16),
            pltpu.VMEM((K, R, W), BF16),
            pltpu.VMEM((K, R, W), BF16),
            pltpu.VMEM((K, R, W), BF16),
            pltpu.VMEM((rows, W), BF16),
            pltpu.VMEM((rows, W), BF16),
            pltpu.VMEM((N_TP, 8, 128), F32),
            pltpu.VMEM((TOK, rows), F32),
            dma((3,)),
            dma((2,)),
            dma((2, N_TP - 1)),
            dma((K,)),
            dma((K, 7)),
            dma((K, 7)),
            dma((K, 4)),
            dma((K, 4)),
            dma((K,)),
            dma((2, N_TP - 1)),
        ],
        compiler_params=pltpu.CompilerParams(collective_id=0, has_side_effects=True, vmem_limit_bytes=48 * 1024 * 1024),
        name="moe_step",
    )(tokens, norm_gain, expert_ids, route_weights, gate_proj, up_proj, down_proj, final_gain)


def solution(mesh):
    placed = (
        P("ep", "tp"),
        P("tp"),
        P("ep", None),
        P("ep", None),
        P("ep", None, "tp"),
        P("ep", None, "tp"),
        P("ep", "tp", None),
        P("tp"),
    )
    return jax.shard_map(step, mesh=mesh, in_specs=placed, out_specs=P("ep", "tp"), check_vma=False)
```

```python
import jax
import jax.numpy as jnp
from jax import lax
from jax.experimental import pallas as pl
from jax.experimental.pallas import tpu as pltpu
from jax.sharding import PartitionSpec as P

MESH = pl.DeviceIdType.MESH
EPSILON = 1e-05
CLAMP_LIMIT = 7.0
SIGMOID_SLOPE = 1.702
F32 = jnp.float32
BF16 = jnp.bfloat16
HIGHEST = lax.Precision.HIGHEST

NZ, NX, NY = 8, 4, 4
N_EP, N_TP = NZ * NX, NY * 2
TOK, CAP, W = 64, 16, 256
D = N_TP * W
ROWS = N_EP * CAP
Z_OFFSETS = (2, 3, 4, 5, 6, 1, 7, 0)
NEAR = 5
R = ROWS // NZ
PER = NX
FAR_ROWS = NEAR * R
NEAR_ROWS = ROWS - FAR_ROWS
GROUPS = ((0, 1), (1, 3), (3, 4), (4, 5), (5, 8))
NEAR_GROUP = len(GROUPS) - 1
SELF = PER * Z_OFFSETS.index(0)
ORDER = (
    "S0 o0 o1 o2", "o3 n1 o4 n0", "f0 n2 f1 n3", "f2 m0 C0 f3",
    "C1 n4 f4 C4", "p0 C2 p1 P0", "C3 p2 p3 F1", "F0 F2 F3",
)


def z_offset(i):
    return Z_OFFSETS[i]


def remote(src, dst, send_sem, recv_sem, ep, tp):
    return pltpu.make_async_remote_copy(
        src_ref=src, dst_ref=dst, send_sem=send_sem, recv_sem=recv_sem, device_id=(ep, tp), device_id_type=MESH
    )


def dot(a, b, dims=((1,), (0,)), precision=None):
    return lax.dot_general(a, b, (dims, ((), ())), precision=precision, preferred_element_type=F32)


def kernel(
    tok_h, ngain_h, ids_h, rw_h, wg_h, wu_h, wd_h, fgain_h, out,
    tbuf, ngain, ids, rw, fgain,
    wg, wu, wd, gbuf, sbuf, snear, xbuf, ps, q, po, ts, tn, ra, rb, rc, obuf, ybuf, ynear, mbuf, nbuf, fbuf, wsel, picks,
    wsem, bulk, gsem, t_sem, n_sem, a_recv, ag_send, ag_recv, rs_send, rs_recv, y_recv, f_sem,
):
    me_ep, me_tp = lax.axis_index("ep"), lax.axis_index("tp")
    z, x = me_ep // NX, lax.rem(me_ep, NX)
    y, c = me_tp // 2, lax.rem(me_tp, 2)
    d = 1 - 2 * c
    co = 1 - c
    yp, ym, yf = lax.rem(y + d + NY, NY), lax.rem(y - d + NY, NY), lax.rem(y + 2, NY)

    def at(yy, cc):
        return yy * 2 + cc

    def back(p):
        return lax.rem(z - z_offset(p // NX) + NZ, NZ) * NX + lax.rem(x - p % NX + NX, NX)

    def forth(p):
        return lax.rem(z + z_offset(p // NX), NZ) * NX + lax.rem(x + p % NX, NX)

    def peer(i):
        return lax.rem(me_tp + i, N_TP)

    def hops(p):
        return min(z_offset(p // NX), NZ - z_offset(p // NX)) + min(p % NX, NX - p % NX)

    far = range(NEAR * PER)
    near = [p for p in range(NEAR * PER, N_EP) if p != SELF]
    barrier = pltpu.get_barrier_semaphore()
    for p in sorted([*far, *near], key=lambda p: -hops(p)):
        pl.semaphore_signal(barrier, inc=1, device_id=(back(p), me_tp), device_id_type=MESH)
    for i in range(1, N_TP):
        pl.semaphore_signal(barrier, inc=1, device_id=(me_ep, peer(i)), device_id_type=MESH)

    small = [
        pltpu.make_async_copy(a, b, wsem.at[3 + i])
        for i, (a, b) in enumerate([(ids_h, ids), (rw_h, rw), (tok_h, tbuf.at[y]), (ngain_h, ngain), (fgain_h, fgain)])
    ]
    loads = [
        pltpu.make_async_copy(wg_h.at[0], wg, wsem.at[0]),
        pltpu.make_async_copy(wu_h.at[0], wu, wsem.at[1]),
        pltpu.make_async_copy(wd_h.at[0], wd, wsem.at[2]),
    ]
    for load in small + loads:
        load.start()
    for load in small:
        load.wait()

    pos = lax.broadcasted_iota(jnp.int32, (N_EP, TOK), 0)
    zi, dx = pos // NX, lax.rem(pos, NX)
    dz = jnp.zeros_like(pos)
    for i, offset in enumerate(Z_OFFSETS):
        dz = jnp.where(zi == i, offset, dz)
    expert = lax.rem(z - dz + 2 * NZ, NZ) * NX + lax.rem(x - dx + NX, NX)
    match = jnp.zeros((N_EP, TOK), F32)
    weight = jnp.zeros((N_EP, TOK), F32)
    for k in range(ids.shape[0]):
        hit = ids[k : k + 1, :] == expert
        match = match + jnp.where(hit, 1.0, 0.0)
        weight = weight + jnp.where(hit, rw[k : k + 1, :], 0.0)
    before = lax.broadcasted_iota(jnp.int32, (TOK, TOK), 0) < lax.broadcasted_iota(jnp.int32, (TOK, TOK), 1)
    earlier = dot(match.astype(BF16), jnp.where(before, 1.0, 0.0).astype(BF16))
    row = lax.broadcasted_iota(jnp.int32, (ROWS, N_EP), 0)
    col = lax.broadcasted_iota(jnp.int32, (ROWS, N_EP), 1)
    spread = jnp.where(row // CAP == col, 1.0, 0.0).astype(BF16)
    slot = lax.rem(lax.broadcasted_iota(jnp.int32, (ROWS, TOK), 0), CAP).astype(F32)
    taken = (dot(spread, earlier.astype(BF16)) == slot) & (dot(spread, match.astype(BF16)) > 0.5)
    picks[...] = jnp.where(taken, 1.0, 0.0).astype(BF16)
    sbuf[...] = dot(picks[0:FAR_ROWS], tbuf[y]).astype(BF16)
    gbuf[me_tp] = jnp.broadcast_to(ngain[...], (8, W))
    with jax.named_scope("barrier"):
        pl.semaphore_wait(barrier, N_EP - 1 + N_TP - 1)

    def block(p):
        return pl.ds(p * CAP, CAP)

    def near_block(p):
        return pl.ds(p * CAP - FAR_ROWS, CAP)

    def chunk(k):
        return pl.ds(k * R, R)

    def group(g):
        lo, hi = GROUPS[g]
        return pl.ds(lo * R, (hi - lo) * R)

    all_far = pl.ds(0, FAR_ROWS)
    all_near = pl.ds(FAR_ROWS, NEAR_ROWS)
    own = SELF * CAP - FAR_ROWS
    parts = (pl.ds(0, own), pl.ds(own + CAP, NEAR_ROWS - own - CAP))
    sends = []

    def send(src, dst, send_sem, recv_sem, tp):
        copy = remote(src, dst, send_sem, recv_sem, me_ep, tp)
        copy.start()
        sends.append(copy)

    def arrived(ref, sem):
        remote(ref, ref, bulk.at[0], sem, me_ep, at(yp, c)).wait_recv()

    for i, yy in enumerate((yf, yp, ym)):
        send(tbuf.at[y], tbuf.at[y], t_sem.at[0, i], t_sem.at[1, i], at(yy, c))
    for p in far:
        remote(sbuf.at[block(p)], xbuf.at[y, c, block(p)], bulk.at[0], a_recv.at[p // PER], back(p), me_tp).start()
    gains = []
    for i in range(1, N_TP):
        gains.append(remote(gbuf.at[me_tp], gbuf.at[me_tp], gsem.at[0, i - 1], gsem.at[1, i - 1], me_ep, peer(i)))
        gains[-1].start()
    sends.extend(gains)

    w_hi = weight.astype(BF16)
    w_lo = (weight - w_hi.astype(F32)).astype(BF16)
    chosen = jnp.where(taken, dot(spread, w_hi) + dot(spread, w_lo), 0.0).T
    c_hi = chosen.astype(BF16)
    wsel[0] = c_hi
    wsel[1] = (chosen - c_hi.astype(F32)).astype(BF16)

    def near_dispatch(_):
        for i, yy in enumerate((yf, ym, yp)):
            arrived(tbuf.at[yy], t_sem.at[1, i])
        for yy in range(NY):
            rows = dot(picks[FAR_ROWS:ROWS], tbuf[yy]).astype(BF16)
            snear[yy] = rows
            xbuf[yy, c, SELF * CAP : (SELF + 1) * CAP] = rows[own : own + CAP]
        for p in near:
            i = int(p > SELF)
            remote(snear.at[:, near_block(p)], xbuf.at[:, c, block(p)], bulk.at[1 + i], a_recv.at[NEAR + i], back(p), me_tp).start()

    def near_share(_):
        for i, span in enumerate(parts):
            ref = xbuf.at[:, c, pl.ds(FAR_ROWS + span.start, span.size)]
            arrived(ref, a_recv.at[NEAR + i])
        ref = xbuf.at[:, c, all_near]
        send(ref, ref, ag_send.at[NEAR, 0], ag_recv.at[NEAR, 0], at(y, co))

    def gather_own(k):
        ref = xbuf.at[y, c, chunk(k)]
        arrived(ref, a_recv.at[k])
        send(ref, ref, ag_send.at[k, 3], ag_recv.at[k, 3], at(yf, c))
        send(ref, ref, ag_send.at[k, 0], ag_recv.at[k, 0], at(yp, c))
        send(ref, ref, ag_send.at[k, 1], ag_recv.at[k, 1], at(ym, c))
        send(ref, ref, ag_send.at[k, 2], ag_recv.at[k, 2], at(y, co))

    def gather_near(k):
        ref = xbuf.at[ym, c, chunk(k)]
        arrived(ref, ag_recv.at[k, 0])
        send(ref, ref, ag_send.at[k, 4], ag_recv.at[k, 4], at(y, co))
        ref = xbuf.at[yp, c, chunk(k)]
        arrived(ref, ag_recv.at[k, 1])
        send(ref, ref, ag_send.at[k, 5], ag_recv.at[k, 5], at(y, co))

    def gather_far(k):
        ref = xbuf.at[yf, c, chunk(k)]
        arrived(ref, ag_recv.at[k, 3])
        send(ref, ref, ag_send.at[k, 6], ag_recv.at[k, 6], at(y, co))

    def compute(g):
        if g == 0:
            for load in loads:
                load.wait()
            for copy in gains:
                copy.wait_recv()
        if g == NEAR_GROUP:
            arrived(xbuf.at[:, co, all_near], ag_recv.at[NEAR, 0])
        else:
            for k in range(*GROUPS[g]):
                for i, yy in ((2, y), (4, yp), (5, ym), (6, yf)):
                    arrived(xbuf.at[yy, co, chunk(k)], ag_recv.at[k, i])
        rows = group(g)
        squares = jnp.zeros((rows.size, W), F32)
        for t in range(N_TP):
            part = xbuf[t // 2, t % 2, rows].astype(F32)
            squares = squares + part * part
        scale = lax.rsqrt(jnp.sum(squares, axis=1, keepdims=True) / D + EPSILON)
        gate = jnp.zeros((rows.size, W), F32)
        up = jnp.zeros((rows.size, W), F32)
        for t in range(N_TP):
            part = xbuf[t // 2, t % 2, rows].astype(F32)
            normed = (part * scale * gbuf[t, 0:1, :]).astype(BF16)
            gate = gate + dot(normed, wg[t * W : (t + 1) * W, :])
            up = up + dot(normed, wu[t * W : (t + 1) * W, :])
        gate = jnp.minimum(gate, CLAMP_LIMIT)
        up = jnp.clip(up, -CLAMP_LIMIT, CLAMP_LIMIT)
        act = ((up + 1.0) * gate * jax.nn.sigmoid(SIGMOID_SLOPE * gate)).astype(BF16)
        for yy in range(NY):
            ps[yy, rows] = dot(act, wd[:, pl.ds(pl.multiple_of(at(yy, co) * W, W), W)]).astype(BF16)
        send(ps.at[:, rows], q.at[:, rows], rs_send.at[g, 0], rs_recv.at[g, 0], at(y, co))
        for yy in range(NY):
            po[yy, rows] = dot(act, wd[:, pl.ds(pl.multiple_of(at(yy, c) * W, W), W)])

    def pair(yy, rows):
        return po[yy, rows] + q[yy, rows].astype(F32)

    def pair_sum(g):
        rows = group(g)
        arrived(q.at[:, rows], rs_recv.at[g, 0])
        for i, (yy, ref) in enumerate(((yf, ra), (ym, rb), (yp, rc))):
            ts[i, rows] = pair(yy, rows).astype(BF16)
            send(ts.at[i, rows], ref.at[rows], rs_send.at[g, 1 + i], rs_recv.at[g, 1 + i], at(yy, c))

    def finish(g):
        rows = group(g)
        total = pair(y, rows)
        for i, ref in ((2, rb), (3, rc), (1, ra)):
            arrived(ref.at[rows], rs_recv.at[g, i])
            total = total + ref[rows].astype(F32)
        obuf[rows] = total.astype(BF16)
        for p in range(GROUPS[g][0] * PER, GROUPS[g][1] * PER):
            remote(obuf.at[block(p)], ybuf.at[block(p)], bulk.at[3], y_recv.at[g], forth(p), me_tp).start()

    def near_return(_):
        arrived(q.at[:, all_near], rs_recv.at[NEAR_GROUP, 0])
        for yy in range(NY):
            rows = pair(yy, all_near).astype(BF16)
            tn[yy] = rows
            ynear[yy, own : own + CAP] = rows[own : own + CAP]
        for p in near:
            i = int(p > SELF)
            remote(tn.at[:, near_block(p)], ynear.at[:, near_block(p)], bulk.at[4 + i], y_recv.at[NEAR_GROUP + i], forth(p), me_tp).start()

    def mixed(columns, values):
        return dot(wsel[0, :, columns], values) + dot(wsel[1, :, columns], values)

    stages = dict(
        S=near_dispatch, m=near_share, o=gather_own, n=gather_near, f=gather_far, C=compute, p=pair_sum, F=finish,
        P=near_return,
    )
    for item in " ".join(ORDER).split():
        with jax.named_scope(item):
            stages[item[0]](int(item[1:]))

    with jax.named_scope("near"):
        for i, span in enumerate(parts):
            arrived(ynear.at[:, span], y_recv.at[NEAR_GROUP + i])
    for i, yy in enumerate((yf, yp, ym)):
        mbuf[i] = mixed(slice(FAR_ROWS, ROWS), ynear[yy]).astype(BF16)
        send(mbuf.at[i], nbuf.at[i], n_sem.at[0, i], n_sem.at[1, i], at(yy, c))
    mixture = mixed(slice(FAR_ROWS, ROWS), ynear[y])
    for g in range(NEAR_GROUP):
        with jax.named_scope(f"return{g}"):
            arrived(ybuf.at[group(g)], y_recv.at[g])
        mixture = mixture + mixed(slice(GROUPS[g][0] * R, GROUPS[g][1] * R), ybuf[group(g)])
    with jax.named_scope("near_sum"):
        for i in range(3):
            arrived(nbuf.at[i], n_sem.at[1, i])
    for i in range(3):
        mixture = mixture + nbuf[i].astype(F32)
    ones = jnp.ones((8, W), F32)
    sums = dot(ones, mixture * mixture, ((1,), (1,)), HIGHEST)
    fbuf[me_tp] = jnp.concatenate([sums, jnp.zeros((8, 128 - TOK), F32)], axis=1)
    finals = []
    for i in (4, 3, 5, 2, 6, 7, 1):
        finals.append(remote(fbuf.at[me_tp], fbuf.at[me_tp], f_sem.at[0, i - 1], f_sem.at[1, i - 1], me_ep, peer(i)))
        finals[-1].start()
    with jax.named_scope("final"):
        for copy in finals:
            copy.wait_recv()
    total = jnp.zeros((8, 128), F32)
    for t in range(N_TP):
        total = total + fbuf[t]
    scale = lax.rsqrt(total / D + EPSILON)
    first = jnp.where(lax.broadcasted_iota(jnp.int32, (8, W), 0) == 0, 1.0, 0.0)
    tall = dot(scale, first, ((0,), (0,)), HIGHEST)[:TOK]
    out[...] = (mixture * tall * fgain[...]).astype(BF16)

    with jax.named_scope("drain"):
        for copy in sends + finals:
            copy.wait_send()
        for i, ref in enumerate(
            (sbuf.at[all_far], snear.at[:, parts[0]], snear.at[:, parts[1]], obuf.at[all_far], tn.at[:, parts[0]], tn.at[:, parts[1]])
        ):
            remote(ref, ref, bulk.at[i], bulk.at[i], me_ep, at(yp, c)).wait_send()


def step(tokens, norm_gain, expert_ids, route_weights, gate_proj, up_proj, down_proj, final_gain):
    vmem = pltpu.VMEM
    dma = pltpu.SemaphoreType.DMA
    groups = len(GROUPS)
    return pl.pallas_call(
        kernel,
        out_shape=jax.ShapeDtypeStruct((TOK, W), BF16),
        in_specs=[pl.BlockSpec(memory_space=pltpu.HBM)] * 8,
        out_specs=pl.BlockSpec(memory_space=vmem),
        scratch_shapes=[
            vmem((NY, TOK, W), BF16),
            vmem((1, W), F32),
            vmem((4, TOK), jnp.int32),
            vmem((4, TOK), F32),
            vmem((1, W), F32),
            vmem((D, W), BF16),
            vmem((D, W), BF16),
            vmem((W, D), BF16),
            vmem((N_TP, 8, W), F32),
            vmem((FAR_ROWS, W), BF16),
            vmem((NY, NEAR_ROWS, W), BF16),
            vmem((NY, 2, ROWS, W), BF16),
            vmem((NY, ROWS, W), BF16),
            vmem((NY, ROWS, W), BF16),
            vmem((NY, ROWS, W), F32),
            vmem((3, FAR_ROWS, W), BF16),
            vmem((NY, NEAR_ROWS, W), BF16),
            vmem((FAR_ROWS, W), BF16),
            vmem((FAR_ROWS, W), BF16),
            vmem((FAR_ROWS, W), BF16),
            vmem((FAR_ROWS, W), BF16),
            vmem((FAR_ROWS, W), BF16),
            vmem((NY, NEAR_ROWS, W), BF16),
            vmem((3, TOK, W), BF16),
            vmem((3, TOK, W), BF16),
            vmem((N_TP, 8, 128), F32),
            vmem((2, TOK, ROWS), BF16),
            vmem((ROWS, TOK), BF16),
            dma((8,)),
            dma((6,)),
            dma((2, N_TP - 1)),
            dma((2, 3)),
            dma((2, 3)),
            dma((NEAR + 2,)),
            dma((NEAR + 1, 7)),
            dma((NEAR + 1, 7)),
            dma((groups, 4)),
            dma((groups, 4)),
            dma((groups + 1,)),
            dma((2, N_TP - 1)),
        ],
        compiler_params=pltpu.CompilerParams(collective_id=0, has_side_effects=True, vmem_limit_bytes=50000000),
        name="moe_step",
    )(*[
        pltpu.with_memory_space_constraint(a, pltpu.HBM)
        for a in (tokens, norm_gain.reshape(1, W), expert_ids.T, route_weights.T, gate_proj, up_proj, down_proj, final_gain.reshape(1, W))
    ])


def solution(mesh):
    placed = (
        P("ep", "tp"),
        P("tp"),
        P("ep", None),
        P("ep", None),
        P("ep", None, "tp"),
        P("ep", None, "tp"),
        P("ep", "tp", None),
        P("tp"),
    )
    return jax.shard_map(step, mesh=mesh, in_specs=placed, out_specs=P("ep", "tp"), check_vma=False)
```

```python
import jax
import jax.numpy as jnp
from jax import lax
from jax.experimental import pallas as pl
from jax.experimental.pallas import tpu as pltpu
from jax.sharding import PartitionSpec as P

MESH = pl.DeviceIdType.MESH
EPSILON = 1e-05
CLAMP_LIMIT = 7.0
SIGMOID_SLOPE = 1.702
F32 = jnp.float32
BF16 = jnp.bfloat16

NZ, NX, NY = 8, 4, 4
N_EP, N_TP = NZ * NX, NY * 2
TOK, CAP, W = 64, 16, 256
D = N_TP * W
ROWS = N_EP * CAP
FAR_Z = (2, 6, 3, 5, 4)
X_OFFSETS = (0, 1, 3, 2)
NEAR_OFFSETS = (
    (1, 0), (7, 0), (1, 1), (7, 3),
    (1, 3), (7, 1), (1, 2), (7, 2),
    (0, 0), (0, 1), (0, 3), (0, 2),
)
NEAR = 5
R = ROWS // NZ
PER = NX
FAR_ROWS = NEAR * R
NEAR_ROWS = ROWS - FAR_ROWS
GROUPS = ((0, 1), (1, 2), (2, 3), (3, 4), (4, 5), (5, 8))
NEAR_GROUP = len(GROUPS) - 1
SELF = PER * NEAR + NEAR_OFFSETS.index((0, 0))
ORDER = (
    "S0 o0 o1 o2", "n0 f0 o3 o4", "n1 f1 m0 n2", "f2 n3 f3 C5",
    "n4 f4 C0 C1", "P0 p0 C2 p1", "C3 p2 C4 p3", "F0 p4 F1 F2",
    "F3 M0 F4",
)


def remote(src, dst, send_sem, recv_sem, ep, tp):
    return pltpu.make_async_remote_copy(
        src_ref=src, dst_ref=dst, send_sem=send_sem, recv_sem=recv_sem, device_id=(ep, tp), device_id_type=MESH
    )


def dot(a, b, dims=((1,), (0,))):
    return lax.dot_general(a, b, (dims, ((), ())), preferred_element_type=F32)


def kernel(
    tok_h, ngain_h, ids_h, rw_h, wg_h, wu_h, wd_h, fgain_h, out,
    tbuf, ngain, ids, rw, fgain,
    wg, wu, wd, gbuf, sbuf, snear, xbuf, ps, q, po, ts, tn, ra, rb, rc, obuf, ybuf, ynear, mbuf, nbuf, fbuf, wsel, picks,
    wsem, bulk, gsem, t_sem, n_sem, a_recv, ag_send, ag_recv, rs_send, rs_recv, y_recv, f_sem,
):
    me_ep, me_tp = lax.axis_index("ep"), lax.axis_index("tp")
    z, x = me_ep // NX, lax.rem(me_ep, NX)
    y, c = me_tp // 2, lax.rem(me_tp, 2)
    d = 1 - 2 * c
    co = 1 - c
    yp, ym, yf = lax.rem(y + d + NY, NY), lax.rem(y - d + NY, NY), lax.rem(y + 2, NY)

    def at(yy, cc):
        return yy * 2 + cc

    def offsets(p):
        return NEAR_OFFSETS[p - NEAR * PER] if p >= NEAR * PER else (FAR_Z[p // PER], X_OFFSETS[p % PER])

    def back(p):
        dz, dx = offsets(p)
        return lax.rem(z - dz + NZ, NZ) * NX + lax.rem(x - dx + NX, NX)

    def forth(p):
        dz, dx = offsets(p)
        return lax.rem(z + dz, NZ) * NX + lax.rem(x + dx, NX)

    def source(g):
        return g + 3 * ((g - z + NZ + 1) // NZ) - 1 + (z + NZ - 1) // NZ + (z + 1) // NZ

    def chunk_of(g):
        past = lax.rem(source(g) - z + NZ, NZ) - 4
        over, under = (past + NZ - 1) // NZ, (NZ - 1 - past) // NZ
        return 4 - 2 * past * (over - under) + over

    def peer(i):
        return lax.rem(me_tp + i, N_TP)

    def hops(p):
        dz, dx = offsets(p)
        return min(dz, NZ - dz) + min(dx, NX - dx)

    far = range(NEAR * PER)
    near = [p for p in range(NEAR * PER, N_EP) if p != SELF]
    barrier = pltpu.get_barrier_semaphore()
    for p in sorted([*far, *near], key=lambda p: -hops(p)):
        pl.semaphore_signal(barrier, inc=1, device_id=(back(p), me_tp), device_id_type=MESH)
    for i in range(1, N_TP):
        pl.semaphore_signal(barrier, inc=1, device_id=(me_ep, peer(i)), device_id_type=MESH)

    small = [
        pltpu.make_async_copy(a, b, wsem.at[3 + i])
        for i, (a, b) in enumerate([(ids_h, ids), (rw_h, rw), (tok_h, tbuf.at[y]), (ngain_h, ngain), (fgain_h, fgain)])
    ]
    loads = [
        pltpu.make_async_copy(wg_h.at[0], wg, wsem.at[0]),
        pltpu.make_async_copy(wu_h.at[0], wu, wsem.at[1]),
        pltpu.make_async_copy(wd_h.at[0], wd, wsem.at[2]),
    ]
    for load in small + loads:
        load.start()
    for load in small:
        load.wait()

    pos = lax.broadcasted_iota(jnp.int32, (N_EP, TOK), 0)
    expert = jnp.zeros_like(pos)
    for p in range(N_EP):
        expert = jnp.where(pos == p, back(p), expert)
    match = jnp.zeros((N_EP, TOK), F32)
    weight = jnp.zeros((N_EP, TOK), F32)
    for k in range(ids.shape[0]):
        hit = ids[k : k + 1, :] == expert
        match = match + jnp.where(hit, 1.0, 0.0)
        weight = weight + jnp.where(hit, rw[k : k + 1, :], 0.0)
    before = lax.broadcasted_iota(jnp.int32, (TOK, TOK), 0) < lax.broadcasted_iota(jnp.int32, (TOK, TOK), 1)
    earlier = dot(match.astype(BF16), jnp.where(before, 1.0, 0.0).astype(BF16))
    row = lax.broadcasted_iota(jnp.int32, (ROWS, N_EP), 0)
    col = lax.broadcasted_iota(jnp.int32, (ROWS, N_EP), 1)
    spread = jnp.where(row // CAP == col, 1.0, 0.0).astype(BF16)
    slot = lax.rem(lax.broadcasted_iota(jnp.int32, (ROWS, TOK), 0), CAP).astype(F32)
    taken = (dot(spread, earlier.astype(BF16)) == slot) & (dot(spread, match.astype(BF16)) > 0.5)
    picks[...] = jnp.where(taken, 1.0, 0.0).astype(BF16)
    sbuf[...] = dot(picks[0:FAR_ROWS], tbuf[y]).astype(BF16)
    gbuf[me_tp] = jnp.broadcast_to(ngain[...], (8, W))
    with jax.named_scope("barrier"):
        pl.semaphore_wait(barrier, N_EP - 1 + N_TP - 1)

    def block(p):
        return pl.ds(p * CAP, CAP)

    def near_block(p):
        return pl.ds(p * CAP - FAR_ROWS, CAP)

    def chunk(k):
        return pl.ds(k * R, R)

    def group(g):
        lo, hi = GROUPS[g]
        return pl.ds(lo * R, (hi - lo) * R)

    all_far = pl.ds(0, FAR_ROWS)
    all_near = pl.ds(FAR_ROWS, NEAR_ROWS)
    own = SELF * CAP - FAR_ROWS
    parts = (pl.ds(0, own), pl.ds(own + CAP, NEAR_ROWS - own - CAP))
    sends = []

    def send(src, dst, send_sem, recv_sem, tp):
        copy = remote(src, dst, send_sem, recv_sem, me_ep, tp)
        copy.start()
        sends.append(copy)

    def arrived(ref, sem):
        remote(ref, ref, bulk.at[0], sem, me_ep, at(yp, c)).wait_recv()

    for i, yy in enumerate((yf, yp, ym)):
        send(tbuf.at[y], tbuf.at[y], t_sem.at[0, i], t_sem.at[1, i], at(yy, c))
    def far_dispatch(positions):
        for p in positions:
            remote(sbuf.at[block(p)], xbuf.at[y, c, block(p)], bulk.at[0], a_recv.at[p // PER], back(p), me_tp).start()

    far_dispatch(far[: 2 * PER])

    @pl.when(c == 0)
    def _():
        far_dispatch(far[2 * PER :])

    gains = []
    for i in range(1, N_TP):
        gains.append(remote(gbuf.at[me_tp], gbuf.at[me_tp], gsem.at[0, i - 1], gsem.at[1, i - 1], me_ep, peer(i)))
        gains[-1].start()
    sends.extend(gains)

    w_hi = weight.astype(BF16)
    w_lo = (weight - w_hi.astype(F32)).astype(BF16)
    chosen = jnp.where(taken, dot(spread, w_hi) + dot(spread, w_lo), 0.0).T
    c_hi = chosen.astype(BF16)
    wsel[0] = c_hi
    wsel[1] = (chosen - c_hi.astype(F32)).astype(BF16)

    def near_dispatch(_):
        arrived(tbuf.at[ym], t_sem.at[1, 1])

        @pl.when(c == 1)
        def _():
            far_dispatch(far[2 * PER :])

        arrived(tbuf.at[yp], t_sem.at[1, 2])
        arrived(tbuf.at[yf], t_sem.at[1, 0])
        for yy in range(NY):
            rows = dot(picks[FAR_ROWS:ROWS], tbuf[yy]).astype(BF16)
            snear[yy] = rows
            xbuf[yy, c, SELF * CAP : (SELF + 1) * CAP] = rows[own : own + CAP]
        for p in near:
            i = int(p > SELF)
            remote(snear.at[:, near_block(p)], xbuf.at[:, c, block(p)], bulk.at[1 + i], a_recv.at[NEAR + i], back(p), me_tp).start()

    def near_share(_):
        for i, span in enumerate(parts):
            ref = xbuf.at[:, c, pl.ds(FAR_ROWS + span.start, span.size)]
            arrived(ref, a_recv.at[NEAR + i])
        ref = xbuf.at[:, c, all_near]
        send(ref, ref, ag_send.at[NEAR, 0], ag_recv.at[NEAR, 0], at(y, co))

    def gather_own(k):
        ref = xbuf.at[y, c, chunk(k)]
        arrived(ref, a_recv.at[k])
        send(ref, ref, ag_send.at[k, 3], ag_recv.at[k, 3], at(yf, c))
        send(ref, ref, ag_send.at[k, 0], ag_recv.at[k, 0], at(yp, c))
        send(ref, ref, ag_send.at[k, 1], ag_recv.at[k, 1], at(ym, c))
        send(ref, ref, ag_send.at[k, 2], ag_recv.at[k, 2], at(y, co))

    def gather_near(k):
        ref = xbuf.at[ym, c, chunk(k)]
        arrived(ref, ag_recv.at[k, 0])
        send(ref, ref, ag_send.at[k, 4], ag_recv.at[k, 4], at(y, co))
        ref = xbuf.at[yp, c, chunk(k)]
        arrived(ref, ag_recv.at[k, 1])
        send(ref, ref, ag_send.at[k, 5], ag_recv.at[k, 5], at(y, co))

    def gather_far(k):
        ref = xbuf.at[yf, c, chunk(k)]
        arrived(ref, ag_recv.at[k, 3])
        send(ref, ref, ag_send.at[k, 6], ag_recv.at[k, 6], at(y, co))

    def compute(g):
        while loads:
            loads.pop().wait()
        for copy in gains[:]:
            copy.wait_recv()
            gains.remove(copy)
        if g == NEAR_GROUP:
            arrived(xbuf.at[:, co, all_near], ag_recv.at[NEAR, 0])
            held = all_near
        else:
            held = pl.ds(pl.multiple_of(chunk_of(g) * R, R), R)
            for i, yy in ((2, y), (4, yp), (5, ym), (6, yf)):
                arrived(xbuf.at[yy, co, held], ag_recv.at[chunk_of(g), i])
        rows = group(g)
        squares = jnp.zeros((rows.size, W), F32)
        for t in range(N_TP):
            part = xbuf[t // 2, t % 2, held].astype(F32)
            squares = squares + part * part
        scale = lax.rsqrt(jnp.sum(squares, axis=1, keepdims=True) / D + EPSILON)
        gate = jnp.zeros((rows.size, W), F32)
        up = jnp.zeros((rows.size, W), F32)
        for t in range(N_TP):
            part = xbuf[t // 2, t % 2, held].astype(F32)
            normed = (part * scale * gbuf[t, 0:1, :]).astype(BF16)
            gate = gate + dot(normed, wg[t * W : (t + 1) * W, :])
            up = up + dot(normed, wu[t * W : (t + 1) * W, :])
        gate = jnp.minimum(gate, CLAMP_LIMIT)
        up = jnp.clip(up, -CLAMP_LIMIT, CLAMP_LIMIT)
        act = ((up + 1.0) * gate * jax.nn.sigmoid(SIGMOID_SLOPE * gate)).astype(BF16)
        for yy in range(NY):
            ps[yy, rows] = dot(act, wd[:, pl.ds(pl.multiple_of(at(yy, co) * W, W), W)]).astype(BF16)
        send(ps.at[:, rows], q.at[:, rows], rs_send.at[g, 0], rs_recv.at[g, 0], at(y, co))
        for yy in range(NY):
            po[yy, rows] = dot(act, wd[:, pl.ds(pl.multiple_of(at(yy, c) * W, W), W)])

    def pair(yy, rows):
        return po[yy, rows] + q[yy, rows].astype(F32)

    def pair_sum(g):
        rows = group(g)
        arrived(q.at[:, rows], rs_recv.at[g, 0])
        for i, (yy, ref) in enumerate(((yf, ra), (ym, rb), (yp, rc))):
            ts[i, rows] = pair(yy, rows).astype(BF16)
            send(ts.at[i, rows], ref.at[rows], rs_send.at[g, 1 + i], rs_recv.at[g, 1 + i], at(yy, c))

    def finish(g):
        rows = group(g)
        total = pair(y, rows)
        for i, ref in ((2, rb), (3, rc), (1, ra)):
            arrived(ref.at[rows], rs_recv.at[g, i])
            total = total + ref[rows].astype(F32)
        obuf[rows] = total.astype(BF16)
        for i, dx in enumerate(X_OFFSETS):
            place = pl.ds(pl.multiple_of(chunk_of(g) * R + i * CAP, CAP), CAP)
            device = source(g) * NX + lax.rem(x + dx, NX)
            remote(obuf.at[block(g * PER + i)], ybuf.at[place], bulk.at[3], y_recv.at[chunk_of(g)], device, me_tp).start()

    def near_return(_):
        arrived(q.at[:, all_near], rs_recv.at[NEAR_GROUP, 0])
        for yy in range(NY):
            rows = pair(yy, all_near).astype(BF16)
            tn[yy] = rows
            ynear[yy, own : own + CAP] = rows[own : own + CAP]
        for p in near:
            i = int(p > SELF)
            remote(tn.at[:, near_block(p)], ynear.at[:, near_block(p)], bulk.at[4 + i], y_recv.at[NEAR + i], forth(p), me_tp).start()

    def mixed(columns, values):
        return dot(wsel[0, :, columns], values) + dot(wsel[1, :, columns], values)

    mixture = []

    def near_mix(_):
        for i, span in enumerate(parts):
            arrived(ynear.at[:, span], y_recv.at[NEAR + i])
        for i, yy in enumerate((yf, yp, ym)):
            mbuf[i] = mixed(slice(FAR_ROWS, ROWS), ynear[yy]).astype(BF16)
            send(mbuf.at[i], nbuf.at[i], n_sem.at[0, i], n_sem.at[1, i], at(yy, c))
        mixture.append(mixed(slice(FAR_ROWS, ROWS), ynear[y]))

    stages = dict(
        S=near_dispatch, m=near_share, o=gather_own, n=gather_near, f=gather_far, C=compute, p=pair_sum, F=finish,
        P=near_return, M=near_mix,
    )
    for item in " ".join(ORDER).split():
        with jax.named_scope(item):
            stages[item[0]](int(item[1:]))

    (mixture,) = mixture
    for k in range(NEAR):
        with jax.named_scope(f"return{k}"):
            arrived(ybuf.at[chunk(k)], y_recv.at[k])
        mixture = mixture + mixed(slice(k * R, (k + 1) * R), ybuf[chunk(k)])
    with jax.named_scope("near_sum"):
        for i in range(3):
            arrived(nbuf.at[i], n_sem.at[1, i])
    for i in range(3):
        mixture = mixture + nbuf[i].astype(F32)

    def halves(a):
        hi = a.astype(BF16)
        return hi, (a - hi.astype(F32)).astype(BF16)

    ones = jnp.ones((8, W), BF16)
    hi, lo = halves(mixture * mixture)
    sums = dot(ones, hi, ((1,), (1,))) + dot(ones, lo, ((1,), (1,)))
    fbuf[me_tp] = jnp.concatenate([sums, jnp.zeros((8, 128 - TOK), F32)], axis=1)
    finals = []
    for i in (4, 3, 5, 2, 6, 7, 1):
        finals.append(remote(fbuf.at[me_tp], fbuf.at[me_tp], f_sem.at[0, i - 1], f_sem.at[1, i - 1], me_ep, peer(i)))
        finals[-1].start()
    with jax.named_scope("final"):
        for copy in finals:
            copy.wait_recv()
    total = jnp.zeros((8, 128), F32)
    for t in range(N_TP):
        total = total + fbuf[t]
    scale = lax.rsqrt(total / D + EPSILON)
    first = jnp.where(lax.broadcasted_iota(jnp.int32, (8, W), 0) == 0, 1.0, 0.0).astype(BF16)
    hi, lo = halves(scale)
    tall = (dot(hi, first, ((0,), (0,))) + dot(lo, first, ((0,), (0,))))[:TOK]
    out[...] = (mixture * tall * fgain[...]).astype(BF16)

    with jax.named_scope("drain"):
        for copy in sends + finals:
            copy.wait_send()
        for i, ref in enumerate(
            (sbuf.at[all_far], snear.at[:, parts[0]], snear.at[:, parts[1]], obuf.at[all_far], tn.at[:, parts[0]], tn.at[:, parts[1]])
        ):
            remote(ref, ref, bulk.at[i], bulk.at[i], me_ep, at(yp, c)).wait_send()


def step(tokens, norm_gain, expert_ids, route_weights, gate_proj, up_proj, down_proj, final_gain):
    vmem = pltpu.VMEM
    dma = pltpu.SemaphoreType.DMA
    groups = len(GROUPS)
    return pl.pallas_call(
        kernel,
        out_shape=jax.ShapeDtypeStruct((TOK, W), BF16),
        in_specs=[pl.BlockSpec(memory_space=pltpu.HBM)] * 8,
        out_specs=pl.BlockSpec(memory_space=vmem),
        scratch_shapes=[
            vmem((NY, TOK, W), BF16),
            vmem((1, W), F32),
            vmem((4, TOK), jnp.int32),
            vmem((4, TOK), F32),
            vmem((1, W), F32),
            vmem((D, W), BF16),
            vmem((D, W), BF16),
            vmem((W, D), BF16),
            vmem((N_TP, 8, W), F32),
            vmem((FAR_ROWS, W), BF16),
            vmem((NY, NEAR_ROWS, W), BF16),
            vmem((NY, 2, ROWS, W), BF16),
            vmem((NY, ROWS, W), BF16),
            vmem((NY, ROWS, W), BF16),
            vmem((NY, ROWS, W), F32),
            vmem((3, FAR_ROWS, W), BF16),
            vmem((NY, NEAR_ROWS, W), BF16),
            vmem((FAR_ROWS, W), BF16),
            vmem((FAR_ROWS, W), BF16),
            vmem((FAR_ROWS, W), BF16),
            vmem((FAR_ROWS, W), BF16),
            vmem((FAR_ROWS, W), BF16),
            vmem((NY, NEAR_ROWS, W), BF16),
            vmem((3, TOK, W), BF16),
            vmem((3, TOK, W), BF16),
            vmem((N_TP, 8, 128), F32),
            vmem((2, TOK, ROWS), BF16),
            vmem((ROWS, TOK), BF16),
            dma((8,)),
            dma((6,)),
            dma((2, N_TP - 1)),
            dma((2, 3)),
            dma((2, 3)),
            dma((NEAR + 2,)),
            dma((NEAR + 1, 7)),
            dma((NEAR + 1, 7)),
            dma((groups, 4)),
            dma((groups, 4)),
            dma((NEAR + 2,)),
            dma((2, N_TP - 1)),
        ],
        compiler_params=pltpu.CompilerParams(collective_id=0, has_side_effects=True, vmem_limit_bytes=50000000),
        name="moe_step",
    )(*[
        pltpu.with_memory_space_constraint(a, pltpu.HBM)
        for a in (tokens, norm_gain.reshape(1, W), expert_ids.T, route_weights.T, gate_proj, up_proj, down_proj, final_gain.reshape(1, W))
    ])


def solution(mesh):
    placed = (
        P("ep", "tp"),
        P("tp"),
        P("ep", None),
        P("ep", None),
        P("ep", None, "tp"),
        P("ep", None, "tp"),
        P("ep", "tp", None),
        P("tp"),
    )
    return jax.shard_map(step, mesh=mesh, in_specs=placed, out_specs=P("ep", "tp"), check_vma=False)
```

```python
import jax
import jax.numpy as jnp
from jax import lax
from jax.experimental import pallas as pl
from jax.experimental.pallas import tpu as pltpu
from jax.sharding import PartitionSpec as P

MESH = pl.DeviceIdType.MESH
EPSILON = 1e-05
CLAMP_LIMIT = 7.0
SIGMOID_SLOPE = 1.702
F32 = jnp.float32
BF16 = jnp.bfloat16

NZ, NX, NY = 8, 4, 4
N_EP, N_TP = NZ * NX, NY * 2
TOK, CAP, W = 64, 16, 256
D = N_TP * W
ROWS = N_EP * CAP
FAR_Z = (2, 6, 3, 5, 4)
X_OFFSETS = (0, 1, 3, 2)
NEAR_OFFSETS = (
    (1, 0), (7, 0), (1, 1), (7, 3),
    (1, 3), (7, 1), (1, 2), (7, 2),
    (0, 0), (0, 1), (0, 3), (0, 2),
)
NEAR = 5
R = ROWS // NZ
PER = NX
FAR_ROWS = NEAR * R
NEAR_ROWS = ROWS - FAR_ROWS
GROUPS = ((0, 1), (1, 2), (2, 3), (3, 4), (4, 5), (5, 8))
NEAR_GROUP = len(GROUPS) - 1
SELF = PER * NEAR + NEAR_OFFSETS.index((0, 0))
ORDER = (
    "S0 o0 o1 o2", "n0 f0 o3 o4", "n1 f1 m0 C0", "n2 f2 n3 f3",
    "C5 p0 n4 f4", "C1 P0 C2 p1", "C3 p2 C4 F0", "p3 p4 F1 F2",
    "F3 M0 F4",
)


def remote(src, dst, send_sem, recv_sem, ep, tp):
    return pltpu.make_async_remote_copy(
        src_ref=src, dst_ref=dst, send_sem=send_sem, recv_sem=recv_sem, device_id=(ep, tp), device_id_type=MESH
    )


def dot(a, b, dims=((1,), (0,))):
    return lax.dot_general(a, b, (dims, ((), ())), preferred_element_type=F32)


def kernel(
    tok_h, ngain_h, ids_h, rw_h, wg_h, wu_h, wd_h, fgain_h, out,
    tbuf, ngain, ids, rw, fgain,
    wg, wu, wd, gbuf, sbuf, snear, xbuf, ps, q, po, ts, tn, ra, rb, rc, obuf, ybuf, ynear, mbuf, nbuf, fbuf, wsel, picks,
    wsem, bulk, gsem, t_sem, n_sem, a_recv, ag_send, ag_recv, rs_send, rs_recv, y_recv, f_sem,
):
    me_ep, me_tp = lax.axis_index("ep"), lax.axis_index("tp")
    z, x = me_ep // NX, lax.rem(me_ep, NX)
    y, c = me_tp // 2, lax.rem(me_tp, 2)
    d = 1 - 2 * c
    co = 1 - c
    yp, ym, yf = lax.rem(y + d + NY, NY), lax.rem(y - d + NY, NY), lax.rem(y + 2, NY)

    def at(yy, cc):
        return yy * 2 + cc

    def offsets(p):
        return NEAR_OFFSETS[p - NEAR * PER] if p >= NEAR * PER else (FAR_Z[p // PER], X_OFFSETS[p % PER])

    def back(p):
        dz, dx = offsets(p)
        return lax.rem(z - dz + NZ, NZ) * NX + lax.rem(x - dx + NX, NX)

    def forth(p):
        dz, dx = offsets(p)
        return lax.rem(z + dz, NZ) * NX + lax.rem(x + dx, NX)

    lead = (z - 2) * ((z + NZ - 3) // NZ) * (1 - (z + 2) // NZ)

    def source(g):
        i = g - 1 + (g - 1 - lead + NZ) // NZ if g else lead
        return i + 3 * ((i - z + NZ + 1) // NZ) - 1 + (z + NZ - 1) // NZ + (z + 1) // NZ

    def chunk_of(g):
        past = lax.rem(source(g) - z + NZ, NZ) - 4
        over, under = (past + NZ - 1) // NZ, (NZ - 1 - past) // NZ
        return 4 - 2 * past * (over - under) + over

    def peer(i):
        return lax.rem(me_tp + i, N_TP)

    def hops(p):
        dz, dx = offsets(p)
        return min(dz, NZ - dz) + min(dx, NX - dx)

    far = range(NEAR * PER)
    near = [p for p in range(NEAR * PER, N_EP) if p != SELF]
    barrier = pltpu.get_barrier_semaphore()
    for p in sorted([*far, *near], key=lambda p: -hops(p)):
        pl.semaphore_signal(barrier, inc=1, device_id=(back(p), me_tp), device_id_type=MESH)
    for i in range(1, N_TP):
        pl.semaphore_signal(barrier, inc=1, device_id=(me_ep, peer(i)), device_id_type=MESH)

    small = [
        pltpu.make_async_copy(a, b, wsem.at[3 + i])
        for i, (a, b) in enumerate([(ids_h, ids), (rw_h, rw), (tok_h, tbuf.at[y]), (ngain_h, ngain), (fgain_h, fgain)])
    ]
    loads = [
        pltpu.make_async_copy(wg_h.at[0], wg, wsem.at[0]),
        pltpu.make_async_copy(wu_h.at[0], wu, wsem.at[1]),
        pltpu.make_async_copy(wd_h.at[0], wd, wsem.at[2]),
    ]
    for load in small + loads:
        load.start()
    for load in small:
        load.wait()

    pos = lax.broadcasted_iota(jnp.int32, (N_EP, TOK), 0)
    expert = jnp.zeros_like(pos)
    for p in range(N_EP):
        expert = jnp.where(pos == p, back(p), expert)
    match = jnp.zeros((N_EP, TOK), F32)
    weight = jnp.zeros((N_EP, TOK), F32)
    for k in range(ids.shape[0]):
        hit = ids[k : k + 1, :] == expert
        match = match + jnp.where(hit, 1.0, 0.0)
        weight = weight + jnp.where(hit, rw[k : k + 1, :], 0.0)
    before = lax.broadcasted_iota(jnp.int32, (TOK, TOK), 0) < lax.broadcasted_iota(jnp.int32, (TOK, TOK), 1)
    earlier = dot(match.astype(BF16), jnp.where(before, 1.0, 0.0).astype(BF16))
    row = lax.broadcasted_iota(jnp.int32, (ROWS, N_EP), 0)
    col = lax.broadcasted_iota(jnp.int32, (ROWS, N_EP), 1)
    spread = jnp.where(row // CAP == col, 1.0, 0.0).astype(BF16)
    slot = lax.rem(lax.broadcasted_iota(jnp.int32, (ROWS, TOK), 0), CAP).astype(F32)
    taken = (dot(spread, earlier.astype(BF16)) == slot) & (dot(spread, match.astype(BF16)) > 0.5)
    picks[...] = jnp.where(taken, 1.0, 0.0).astype(BF16)
    sbuf[...] = dot(picks[0:FAR_ROWS], tbuf[y]).astype(BF16)
    gbuf[me_tp] = jnp.broadcast_to(ngain[...], (8, W))
    with jax.named_scope("barrier"):
        pl.semaphore_wait(barrier, N_EP - 1 + N_TP - 1)

    def block(p):
        return pl.ds(p * CAP, CAP)

    def near_block(p):
        return pl.ds(p * CAP - FAR_ROWS, CAP)

    def chunk(k):
        return pl.ds(k * R, R)

    def group(g):
        lo, hi = GROUPS[g]
        return pl.ds(lo * R, (hi - lo) * R)

    all_far = pl.ds(0, FAR_ROWS)
    all_near = pl.ds(FAR_ROWS, NEAR_ROWS)
    own = SELF * CAP - FAR_ROWS
    parts = (pl.ds(0, own), pl.ds(own + CAP, NEAR_ROWS - own - CAP))
    sends = []

    def send(src, dst, send_sem, recv_sem, tp):
        copy = remote(src, dst, send_sem, recv_sem, me_ep, tp)
        copy.start()
        sends.append(copy)

    def arrived(ref, sem):
        remote(ref, ref, bulk.at[0], sem, me_ep, at(yp, c)).wait_recv()

    for i, yy in enumerate((yf, yp, ym)):
        send(tbuf.at[y], tbuf.at[y], t_sem.at[0, i], t_sem.at[1, i], at(yy, c))
    def far_dispatch(positions):
        for p in positions:
            remote(sbuf.at[block(p)], xbuf.at[y, c, block(p)], bulk.at[0], a_recv.at[p // PER], back(p), me_tp).start()

    far_dispatch(far[: 2 * PER])

    @pl.when(c == 0)
    def _():
        far_dispatch(far[2 * PER :])

    gains = []
    for i in range(1, N_TP):
        gains.append(remote(gbuf.at[me_tp], gbuf.at[me_tp], gsem.at[0, i - 1], gsem.at[1, i - 1], me_ep, peer(i)))
        gains[-1].start()
    sends.extend(gains)

    w_hi = weight.astype(BF16)
    w_lo = (weight - w_hi.astype(F32)).astype(BF16)
    chosen = jnp.where(taken, dot(spread, w_hi) + dot(spread, w_lo), 0.0).T
    c_hi = chosen.astype(BF16)
    wsel[0] = c_hi
    wsel[1] = (chosen - c_hi.astype(F32)).astype(BF16)

    def near_dispatch(_):
        arrived(tbuf.at[ym], t_sem.at[1, 1])

        @pl.when(c == 1)
        def _():
            far_dispatch(far[2 * PER :])

        arrived(tbuf.at[yp], t_sem.at[1, 2])
        arrived(tbuf.at[yf], t_sem.at[1, 0])
        for yy in range(NY):
            rows = dot(picks[FAR_ROWS:ROWS], tbuf[yy]).astype(BF16)
            snear[yy] = rows
            xbuf[yy, c, SELF * CAP : (SELF + 1) * CAP] = rows[own : own + CAP]
        for p in near:
            i = int(p > SELF)
            remote(snear.at[:, near_block(p)], xbuf.at[:, c, block(p)], bulk.at[1 + i], a_recv.at[NEAR + i], back(p), me_tp).start()

    def near_share(_):
        for i, span in enumerate(parts):
            ref = xbuf.at[:, c, pl.ds(FAR_ROWS + span.start, span.size)]
            arrived(ref, a_recv.at[NEAR + i])
        ref = xbuf.at[:, c, all_near]
        send(ref, ref, ag_send.at[NEAR, 0], ag_recv.at[NEAR, 0], at(y, co))

    def gather_own(k):
        ref = xbuf.at[y, c, chunk(k)]
        arrived(ref, a_recv.at[k])
        send(ref, ref, ag_send.at[k, 3], ag_recv.at[k, 3], at(yf, c))
        send(ref, ref, ag_send.at[k, 0], ag_recv.at[k, 0], at(yp, c))
        send(ref, ref, ag_send.at[k, 1], ag_recv.at[k, 1], at(ym, c))
        send(ref, ref, ag_send.at[k, 2], ag_recv.at[k, 2], at(y, co))

    def gather_near(k):
        ref = xbuf.at[ym, c, chunk(k)]
        arrived(ref, ag_recv.at[k, 0])
        send(ref, ref, ag_send.at[k, 4], ag_recv.at[k, 4], at(y, co))
        ref = xbuf.at[yp, c, chunk(k)]
        arrived(ref, ag_recv.at[k, 1])
        send(ref, ref, ag_send.at[k, 5], ag_recv.at[k, 5], at(y, co))

    def gather_far(k):
        ref = xbuf.at[yf, c, chunk(k)]
        arrived(ref, ag_recv.at[k, 3])
        send(ref, ref, ag_send.at[k, 6], ag_recv.at[k, 6], at(y, co))

    def compute(g):
        while loads:
            loads.pop().wait()
        for copy in gains[:]:
            copy.wait_recv()
            gains.remove(copy)
        if g == NEAR_GROUP:
            arrived(xbuf.at[:, co, all_near], ag_recv.at[NEAR, 0])
            held = all_near
        else:
            held = pl.ds(pl.multiple_of(chunk_of(g) * R, R), R)
            for i, yy in ((2, y), (4, yp), (5, ym), (6, yf)):
                arrived(xbuf.at[yy, co, held], ag_recv.at[chunk_of(g), i])
        rows = group(g)
        squares = jnp.zeros((rows.size, W), F32)
        for t in range(N_TP):
            part = xbuf[t // 2, t % 2, held].astype(F32)
            squares = squares + part * part
        scale = lax.rsqrt(jnp.sum(squares, axis=1, keepdims=True) / D + EPSILON)
        gate = jnp.zeros((rows.size, W), F32)
        up = jnp.zeros((rows.size, W), F32)
        for t in range(N_TP):
            part = xbuf[t // 2, t % 2, held].astype(F32)
            normed = (part * scale * gbuf[t, 0:1, :]).astype(BF16)
            gate = gate + dot(normed, wg[t * W : (t + 1) * W, :])
            up = up + dot(normed, wu[t * W : (t + 1) * W, :])
        gate = jnp.minimum(gate, CLAMP_LIMIT)
        up = jnp.clip(up, -CLAMP_LIMIT, CLAMP_LIMIT)
        act = ((up + 1.0) * gate * jax.nn.sigmoid(SIGMOID_SLOPE * gate)).astype(BF16)
        for yy in range(NY):
            ps[yy, rows] = dot(act, wd[:, pl.ds(pl.multiple_of(at(yy, co) * W, W), W)]).astype(BF16)
        send(ps.at[:, rows], q.at[:, rows], rs_send.at[g, 0], rs_recv.at[g, 0], at(y, co))
        for yy in range(NY):
            po[yy, rows] = dot(act, wd[:, pl.ds(pl.multiple_of(at(yy, c) * W, W), W)])

    def pair(yy, rows):
        return po[yy, rows] + q[yy, rows].astype(F32)

    def pair_sum(g):
        rows = group(g)
        arrived(q.at[:, rows], rs_recv.at[g, 0])
        for i, (yy, ref) in enumerate(((yf, ra), (ym, rb), (yp, rc))):
            ts[i, rows] = pair(yy, rows).astype(BF16)
            send(ts.at[i, rows], ref.at[rows], rs_send.at[g, 1 + i], rs_recv.at[g, 1 + i], at(yy, c))

    def finish(g):
        rows = group(g)
        total = pair(y, rows)
        for i, ref in ((2, rb), (3, rc), (1, ra)):
            arrived(ref.at[rows], rs_recv.at[g, i])
            total = total + ref[rows].astype(F32)
        obuf[rows] = total.astype(BF16)
        for i, dx in enumerate(X_OFFSETS):
            place = pl.ds(pl.multiple_of(chunk_of(g) * R + i * CAP, CAP), CAP)
            device = source(g) * NX + lax.rem(x + dx, NX)
            remote(obuf.at[block(g * PER + i)], ybuf.at[place], bulk.at[3], y_recv.at[chunk_of(g)], device, me_tp).start()

    def near_return(_):
        arrived(q.at[:, all_near], rs_recv.at[NEAR_GROUP, 0])
        for yy in range(NY):
            rows = pair(yy, all_near).astype(BF16)
            tn[yy] = rows
            ynear[yy, own : own + CAP] = rows[own : own + CAP]
        for p in near:
            i = int(p > SELF)
            remote(tn.at[:, near_block(p)], ynear.at[:, near_block(p)], bulk.at[4 + i], y_recv.at[NEAR + i], forth(p), me_tp).start()

    def mixed(columns, values):
        return dot(wsel[0, :, columns], values) + dot(wsel[1, :, columns], values)

    mixture = []

    def near_mix(_):
        for i, span in enumerate(parts):
            arrived(ynear.at[:, span], y_recv.at[NEAR + i])
        for i, yy in enumerate((yf, yp, ym)):
            mbuf[i] = mixed(slice(FAR_ROWS, ROWS), ynear[yy]).astype(BF16)
            send(mbuf.at[i], nbuf.at[i], n_sem.at[0, i], n_sem.at[1, i], at(yy, c))
        mixture.append(mixed(slice(FAR_ROWS, ROWS), ynear[y]))

    stages = dict(
        S=near_dispatch, m=near_share, o=gather_own, n=gather_near, f=gather_far, C=compute, p=pair_sum, F=finish,
        P=near_return, M=near_mix,
    )
    for item in " ".join(ORDER).split():
        with jax.named_scope(item):
            stages[item[0]](int(item[1:]))

    (mixture,) = mixture
    for k in range(NEAR):
        with jax.named_scope(f"return{k}"):
            arrived(ybuf.at[chunk(k)], y_recv.at[k])
        mixture = mixture + mixed(slice(k * R, (k + 1) * R), ybuf[chunk(k)])
    with jax.named_scope("near_sum"):
        for i in range(3):
            arrived(nbuf.at[i], n_sem.at[1, i])
    for i in range(3):
        mixture = mixture + nbuf[i].astype(F32)

    def halves(a):
        hi = a.astype(BF16)
        return hi, (a - hi.astype(F32)).astype(BF16)

    ones = jnp.ones((8, W), BF16)
    hi, lo = halves(mixture * mixture)
    sums = dot(ones, hi, ((1,), (1,))) + dot(ones, lo, ((1,), (1,)))
    fbuf[me_tp] = jnp.concatenate([sums, jnp.zeros((8, 128 - TOK), F32)], axis=1)
    finals = []
    for i in (4, 3, 5, 2, 6, 7, 1):
        finals.append(remote(fbuf.at[me_tp], fbuf.at[me_tp], f_sem.at[0, i - 1], f_sem.at[1, i - 1], me_ep, peer(i)))
        finals[-1].start()
    with jax.named_scope("final"):
        for copy in finals:
            copy.wait_recv()
    total = jnp.zeros((8, 128), F32)
    for t in range(N_TP):
        total = total + fbuf[t]
    scale = lax.rsqrt(total / D + EPSILON)
    first = jnp.where(lax.broadcasted_iota(jnp.int32, (8, W), 0) == 0, 1.0, 0.0).astype(BF16)
    hi, lo = halves(scale)
    tall = (dot(hi, first, ((0,), (0,))) + dot(lo, first, ((0,), (0,))))[:TOK]
    out[...] = (mixture * tall * fgain[...]).astype(BF16)

    with jax.named_scope("drain"):
        for copy in sends + finals:
            copy.wait_send()
        for i, ref in enumerate(
            (sbuf.at[all_far], snear.at[:, parts[0]], snear.at[:, parts[1]], obuf.at[all_far], tn.at[:, parts[0]], tn.at[:, parts[1]])
        ):
            remote(ref, ref, bulk.at[i], bulk.at[i], me_ep, at(yp, c)).wait_send()


def step(tokens, norm_gain, expert_ids, route_weights, gate_proj, up_proj, down_proj, final_gain):
    vmem = pltpu.VMEM
    dma = pltpu.SemaphoreType.DMA
    groups = len(GROUPS)
    return pl.pallas_call(
        kernel,
        out_shape=jax.ShapeDtypeStruct((TOK, W), BF16),
        in_specs=[pl.BlockSpec(memory_space=pltpu.HBM)] * 8,
        out_specs=pl.BlockSpec(memory_space=vmem),
        scratch_shapes=[
            vmem((NY, TOK, W), BF16),
            vmem((1, W), F32),
            vmem((4, TOK), jnp.int32),
            vmem((4, TOK), F32),
            vmem((1, W), F32),
            vmem((D, W), BF16),
            vmem((D, W), BF16),
            vmem((W, D), BF16),
            vmem((N_TP, 8, W), F32),
            vmem((FAR_ROWS, W), BF16),
            vmem((NY, NEAR_ROWS, W), BF16),
            vmem((NY, 2, ROWS, W), BF16),
            vmem((NY, ROWS, W), BF16),
            vmem((NY, ROWS, W), BF16),
            vmem((NY, ROWS, W), F32),
            vmem((3, FAR_ROWS, W), BF16),
            vmem((NY, NEAR_ROWS, W), BF16),
            vmem((FAR_ROWS, W), BF16),
            vmem((FAR_ROWS, W), BF16),
            vmem((FAR_ROWS, W), BF16),
            vmem((FAR_ROWS, W), BF16),
            vmem((FAR_ROWS, W), BF16),
            vmem((NY, NEAR_ROWS, W), BF16),
            vmem((3, TOK, W), BF16),
            vmem((3, TOK, W), BF16),
            vmem((N_TP, 8, 128), F32),
            vmem((2, TOK, ROWS), BF16),
            vmem((ROWS, TOK), BF16),
            dma((8,)),
            dma((6,)),
            dma((2, N_TP - 1)),
            dma((2, 3)),
            dma((2, 3)),
            dma((NEAR + 2,)),
            dma((NEAR + 1, 7)),
            dma((NEAR + 1, 7)),
            dma((groups, 4)),
            dma((groups, 4)),
            dma((NEAR + 2,)),
            dma((2, N_TP - 1)),
        ],
        compiler_params=pltpu.CompilerParams(collective_id=0, has_side_effects=True, vmem_limit_bytes=50000000),
        name="moe_step",
    )(*[
        pltpu.with_memory_space_constraint(a, pltpu.HBM)
        for a in (tokens, norm_gain.reshape(1, W), expert_ids.T, route_weights.T, gate_proj, up_proj, down_proj, final_gain.reshape(1, W))
    ])


def solution(mesh):
    placed = (
        P("ep", "tp"),
        P("tp"),
        P("ep", None),
        P("ep", None),
        P("ep", None, "tp"),
        P("ep", None, "tp"),
        P("ep", "tp", None),
        P("tp"),
    )
    return jax.shard_map(step, mesh=mesh, in_specs=placed, out_specs=P("ep", "tp"), check_vma=False)
```

```python
import jax
import jax.numpy as jnp
from jax import lax
from jax.experimental import pallas as pl
from jax.experimental.pallas import tpu as pltpu
from jax.sharding import PartitionSpec as P

MESH = pl.DeviceIdType.MESH
EPSILON = 1e-05
CLAMP_LIMIT = 7.0
SIGMOID_SLOPE = 1.702
F32 = jnp.float32
BF16 = jnp.bfloat16

NZ, NX, NY = 8, 4, 4
N_EP, N_TP = NZ * NX, NY * 2
TOK, CAP, W = 64, 16, 256
D = N_TP * W
ROWS = N_EP * CAP
FAR_Z = (2, 6, 3, 5, 4)
X_OFFSETS = (0, 1, 3, 2)
NEAR_OFFSETS = (
    (1, 0), (7, 0), (1, 1), (7, 3),
    (1, 3), (7, 1), (1, 2), (7, 2),
    (0, 0), (0, 1), (0, 3), (0, 2),
)
NEAR = 5
R = ROWS // NZ
PER = NX
FAR_ROWS = NEAR * R
NEAR_ROWS = ROWS - FAR_ROWS
GROUPS = ((0, 1), (1, 2), (2, 3), (3, 4), (4, 5), (5, 8))
NEAR_GROUP = len(GROUPS) - 1
SELF = PER * NEAR + NEAR_OFFSETS.index((0, 0))
ORDER = (
    "S0 o0 o1 o2", "n0 f0 o3 o4", "n1 f1 m0 C0", "n2 f2 n3 f3",
    "C5 p0 n4 f4", "C1 P0 C2 p1", "C3 p2 C4 F0", "p3 p4 F1 F2",
    "F3 M0 F4",
)


def remote(src, dst, send_sem, recv_sem, ep, tp):
    return pltpu.make_async_remote_copy(
        src_ref=src, dst_ref=dst, send_sem=send_sem, recv_sem=recv_sem, device_id=(ep, tp), device_id_type=MESH
    )


def dot(a, b, dims=((1,), (0,))):
    return lax.dot_general(a, b, (dims, ((), ())), preferred_element_type=F32)


def kernel(
    tok_h, ngain_h, ids_h, rw_h, wg_h, wu_h, wd_h, fgain_h, out,
    tbuf, ids, rw, fgain,
    wg, wu, wd, gbuf, sbuf, snear, xbuf, ps, q, po, ts, tn, rbuf, obuf, ybuf, ynear, mbuf, nbuf, fbuf, wsel, picks,
    wsem, bulk, gsem, t_sem, n_sem, a_recv, ag_send, ag_recv, rs_send, rs_recv, y_recv, f_sem,
):
    me_ep, me_tp = lax.axis_index("ep"), lax.axis_index("tp")
    z, x = me_ep // NX, lax.rem(me_ep, NX)
    y, c = me_tp // 2, lax.rem(me_tp, 2)
    d = 1 - 2 * c
    co = 1 - c
    yp, ym, yf = lax.rem(y + d + NY, NY), lax.rem(y - d + NY, NY), lax.rem(y + 2, NY)

    def at(yy, cc):
        return yy * 2 + cc

    def offsets(p):
        return NEAR_OFFSETS[p - NEAR * PER] if p >= NEAR * PER else (FAR_Z[p // PER], X_OFFSETS[p % PER])

    def back(p):
        dz, dx = offsets(p)
        return lax.rem(z - dz + NZ, NZ) * NX + lax.rem(x - dx + NX, NX)

    def forth(p):
        dz, dx = offsets(p)
        return lax.rem(z + dz, NZ) * NX + lax.rem(x + dx, NX)

    lead = (z - 2) * ((z + NZ - 3) // NZ) * (1 - (z + 2) // NZ)

    def source(g):
        i = g - 1 + (g - 1 - lead + NZ) // NZ if g else lead
        return i + 3 * ((i - z + NZ + 1) // NZ) - 1 + (z + NZ - 1) // NZ + (z + 1) // NZ

    def chunk_of(g):
        past = lax.rem(source(g) - z + NZ, NZ) - 4
        over, under = (past + NZ - 1) // NZ, (NZ - 1 - past) // NZ
        return 4 - 2 * past * (over - under) + over

    def peer(i):
        return lax.rem(me_tp + i, N_TP)

    def hops(p):
        dz, dx = offsets(p)
        return min(dz, NZ - dz) + min(dx, NX - dx)

    far = range(NEAR * PER)
    near = [p for p in range(NEAR * PER, N_EP) if p != SELF]
    barrier = pltpu.get_barrier_semaphore()
    for p in sorted([*far, *near], key=lambda p: -hops(p)):
        pl.semaphore_signal(barrier, inc=1, device_id=(back(p), me_tp), device_id_type=MESH)
    for i in range(1, N_TP):
        pl.semaphore_signal(barrier, inc=1, device_id=(me_ep, peer(i)), device_id_type=MESH)

    small = [
        pltpu.make_async_copy(a, b, wsem.at[3 + i])
        for i, (a, b) in enumerate([(ids_h, ids), (rw_h, rw), (tok_h, tbuf.at[y]), (ngain_h, gbuf.at[me_tp]), (fgain_h, fgain)])
    ]
    loads = [
        pltpu.make_async_copy(wg_h.at[0], wg, wsem.at[0]),
        pltpu.make_async_copy(wu_h.at[0], wu, wsem.at[1]),
        pltpu.make_async_copy(wd_h.at[0], wd, wsem.at[2]),
    ]
    for load in small + loads:
        load.start()
    for load in small:
        load.wait()

    pos = lax.broadcasted_iota(jnp.int32, (N_EP, TOK), 0)
    expert = jnp.zeros_like(pos)
    for p in range(N_EP):
        expert = jnp.where(pos == p, back(p), expert)
    match = jnp.zeros((N_EP, TOK), F32)
    weight = jnp.zeros((N_EP, TOK), F32)
    for k in range(ids.shape[0]):
        hit = ids[k : k + 1, :] == expert
        match = match + jnp.where(hit, 1.0, 0.0)
        weight = weight + jnp.where(hit, rw[k : k + 1, :], 0.0)
    before = lax.broadcasted_iota(jnp.int32, (TOK, TOK), 0) < lax.broadcasted_iota(jnp.int32, (TOK, TOK), 1)
    earlier = dot(match.astype(BF16), jnp.where(before, 1.0, 0.0).astype(BF16))
    row = lax.broadcasted_iota(jnp.int32, (ROWS, N_EP), 0)
    col = lax.broadcasted_iota(jnp.int32, (ROWS, N_EP), 1)
    spread = jnp.where(row // CAP == col, 1.0, 0.0).astype(BF16)
    slot = lax.rem(lax.broadcasted_iota(jnp.int32, (ROWS, TOK), 0), CAP).astype(F32)
    taken = (dot(spread, earlier.astype(BF16)) == slot) & (dot(spread, match.astype(BF16)) > 0.5)
    picks[...] = jnp.where(taken, 1.0, 0.0).astype(BF16)
    sbuf[...] = dot(picks[0:FAR_ROWS], tbuf[y]).astype(BF16)
    with jax.named_scope("barrier"):
        pl.semaphore_wait(barrier, N_EP - 1 + N_TP - 1)

    def block(p):
        return pl.ds(p * CAP, CAP)

    def near_block(p):
        return pl.ds(p * CAP - FAR_ROWS, CAP)

    def chunk(k):
        return pl.ds(k * R, R)

    def group(g):
        lo, hi = GROUPS[g]
        return pl.ds(lo * R, (hi - lo) * R)

    all_far = pl.ds(0, FAR_ROWS)
    all_near = pl.ds(FAR_ROWS, NEAR_ROWS)
    own = SELF * CAP - FAR_ROWS
    parts = (pl.ds(0, own), pl.ds(own + CAP, NEAR_ROWS - own - CAP))
    def send(src, dst, send_sem, recv_sem, tp):
        remote(src, dst, send_sem, recv_sem, me_ep, tp).start()

    def arrived(ref, sem):
        remote(ref, ref, bulk.at[0], sem, me_ep, at(yp, c)).wait_recv()

    for i, yy in enumerate((yf, yp, ym)):
        send(tbuf.at[y], tbuf.at[y], t_sem.at[0], t_sem.at[1 + i], at(yy, c))
    def far_dispatch(positions):
        for p in positions:
            remote(sbuf.at[block(p)], xbuf.at[y, c, block(p)], bulk.at[0], a_recv.at[p // PER], back(p), me_tp).start()

    far_dispatch(far[: 2 * PER])

    @pl.when(c == 0)
    def _():
        far_dispatch(far[2 * PER :])

    for i in range(1, N_TP):
        send(gbuf.at[me_tp], gbuf.at[me_tp], gsem.at[0], gsem.at[1], peer(i))

    w_hi = weight.astype(BF16)
    w_lo = (weight - w_hi.astype(F32)).astype(BF16)
    chosen = jnp.where(taken, dot(spread, w_hi) + dot(spread, w_lo), 0.0).T
    c_hi = chosen.astype(BF16)
    wsel[0] = c_hi
    wsel[1] = (chosen - c_hi.astype(F32)).astype(BF16)

    def near_dispatch(_):
        arrived(tbuf.at[ym], t_sem.at[2])

        @pl.when(c == 1)
        def _():
            far_dispatch(far[2 * PER :])

        arrived(tbuf.at[yp], t_sem.at[3])
        arrived(tbuf.at[yf], t_sem.at[1])
        for yy in range(NY):
            rows = dot(picks[FAR_ROWS:ROWS], tbuf[yy]).astype(BF16)
            snear[yy] = rows
            xbuf[yy, c, SELF * CAP : (SELF + 1) * CAP] = rows[own : own + CAP]
        for p in near:
            i = int(p > SELF)
            remote(snear.at[:, near_block(p)], xbuf.at[:, c, block(p)], bulk.at[1 + i], a_recv.at[NEAR + i], back(p), me_tp).start()

    def near_share(_):
        for i, span in enumerate(parts):
            ref = xbuf.at[:, c, pl.ds(FAR_ROWS + span.start, span.size)]
            arrived(ref, a_recv.at[NEAR + i])
        ref = xbuf.at[:, c, all_near]
        send(ref, ref, ag_send.at[NEAR], ag_recv.at[NEAR, 3], at(y, co))

    def gather_own(k):
        ref = xbuf.at[y, c, chunk(k)]
        arrived(ref, a_recv.at[k])
        for i, tp in ((2, at(yf, c)), (0, at(yp, c)), (1, at(ym, c)), (3, at(y, co))):
            send(ref, ref, ag_send.at[k], ag_recv.at[k, i], tp)

    def gather_near(k):
        ref = xbuf.at[ym, c, chunk(k)]
        arrived(ref, ag_recv.at[k, 0])
        send(ref, ref, ag_send.at[k], ag_recv.at[k, 3], at(y, co))
        ref = xbuf.at[yp, c, chunk(k)]
        arrived(ref, ag_recv.at[k, 1])
        send(ref, ref, ag_send.at[k], ag_recv.at[k, 3], at(y, co))

    def gather_far(k):
        ref = xbuf.at[yf, c, chunk(k)]
        arrived(ref, ag_recv.at[k, 2])
        send(ref, ref, ag_send.at[k], ag_recv.at[k, 3], at(y, co))

    def compute(g):
        if loads:
            arrived(gbuf.at[pl.ds(0, N_TP - 1)], gsem.at[1])
        while loads:
            loads.pop().wait()
        if g == NEAR_GROUP:
            arrived(xbuf.at[:, co, all_near], ag_recv.at[NEAR, 3])
            held = all_near
        else:
            held = pl.ds(pl.multiple_of(chunk_of(g) * R, R), R)
            arrived(xbuf.at[:, co, held], ag_recv.at[chunk_of(g), 3])
        rows = group(g)
        squares = jnp.zeros((rows.size, W), F32)
        for t in range(N_TP):
            part = xbuf[t // 2, t % 2, held].astype(F32)
            squares = squares + part * part
        scale = lax.rsqrt(jnp.sum(squares, axis=1, keepdims=True) / D + EPSILON)
        gate = jnp.zeros((rows.size, W), F32)
        up = jnp.zeros((rows.size, W), F32)
        for t in range(N_TP):
            part = xbuf[t // 2, t % 2, held].astype(F32)
            normed = (part * scale * gbuf[t]).astype(BF16)
            gate = gate + dot(normed, wg[t * W : (t + 1) * W, :])
            up = up + dot(normed, wu[t * W : (t + 1) * W, :])
        gate = jnp.minimum(gate, CLAMP_LIMIT)
        up = jnp.clip(up, -CLAMP_LIMIT, CLAMP_LIMIT)
        act = ((up + 1.0) * gate * jax.nn.sigmoid(SIGMOID_SLOPE * gate)).astype(BF16)
        for yy in range(NY):
            ps[yy, rows] = dot(act, wd[:, pl.ds(pl.multiple_of(at(yy, co) * W, W), W)]).astype(BF16)
        send(ps.at[:, rows], q.at[:, rows], rs_send.at[g], rs_recv.at[g, 0], at(y, co))
        for yy in range(NY):
            po[yy, rows] = dot(act, wd[:, pl.ds(pl.multiple_of(at(yy, c) * W, W), W)])

    def pair(yy, rows):
        return po[yy, rows] + q[yy, rows].astype(F32)

    def pair_sum(g):
        rows = group(g)
        arrived(q.at[:, rows], rs_recv.at[g, 0])
        for i, yy in enumerate((yf, ym, yp)):
            ts[i, rows] = pair(yy, rows).astype(BF16)
            send(ts.at[i, rows], rbuf.at[i, rows], rs_send.at[g], rs_recv.at[g, 1], at(yy, c))

    def finish(g):
        rows = group(g)
        total = pair(y, rows)
        arrived(rbuf.at[:, rows], rs_recv.at[g, 1])
        for i in range(3):
            total = total + rbuf[i, rows].astype(F32)
        obuf[rows] = total.astype(BF16)
        for i, dx in enumerate(X_OFFSETS):
            place = pl.ds(pl.multiple_of(chunk_of(g) * R + i * CAP, CAP), CAP)
            device = source(g) * NX + lax.rem(x + dx, NX)
            remote(obuf.at[block(g * PER + i)], ybuf.at[place], bulk.at[3], y_recv.at[chunk_of(g)], device, me_tp).start()

    def near_return(_):
        arrived(q.at[:, all_near], rs_recv.at[NEAR_GROUP, 0])
        for yy in range(NY):
            rows = pair(yy, all_near).astype(BF16)
            tn[yy] = rows
            ynear[yy, own : own + CAP] = rows[own : own + CAP]
        for p in near:
            i = int(p > SELF)
            remote(tn.at[:, near_block(p)], ynear.at[:, near_block(p)], bulk.at[4 + i], y_recv.at[NEAR + i], forth(p), me_tp).start()

    def mixed(columns, values):
        return dot(wsel[0, :, columns], values) + dot(wsel[1, :, columns], values)

    mixture = []

    def near_mix(_):
        for i, span in enumerate(parts):
            arrived(ynear.at[:, span], y_recv.at[NEAR + i])
        for i, yy in enumerate((yf, yp, ym)):
            mbuf[i] = mixed(slice(FAR_ROWS, ROWS), ynear[yy]).astype(BF16)
            send(mbuf.at[i], nbuf.at[i], n_sem.at[0], n_sem.at[1], at(yy, c))
        mixture.append(mixed(slice(FAR_ROWS, ROWS), ynear[y]))

    stages = dict(
        S=near_dispatch, m=near_share, o=gather_own, n=gather_near, f=gather_far, C=compute, p=pair_sum, F=finish,
        P=near_return, M=near_mix,
    )
    for item in " ".join(ORDER).split():
        with jax.named_scope(item):
            stages[item[0]](int(item[1:]))

    (mixture,) = mixture
    for k in range(NEAR):
        with jax.named_scope(f"return{k}"):
            arrived(ybuf.at[chunk(k)], y_recv.at[k])
        mixture = mixture + mixed(slice(k * R, (k + 1) * R), ybuf[chunk(k)])
    with jax.named_scope("near_sum"):
        arrived(nbuf, n_sem.at[1])
    for i in range(3):
        mixture = mixture + nbuf[i].astype(F32)

    def halves(a):
        hi = a.astype(BF16)
        return hi, (a - hi.astype(F32)).astype(BF16)

    ones = jnp.ones((8, W), BF16)
    hi, lo = halves(mixture * mixture)
    sums = dot(ones, hi, ((1,), (1,))) + dot(ones, lo, ((1,), (1,)))
    fbuf[me_tp] = jnp.concatenate([sums, jnp.zeros((8, 128 - TOK), F32)], axis=1)[0:1]
    for i in (4, 3, 5, 2, 6, 7, 1):
        send(fbuf.at[me_tp], fbuf.at[me_tp], f_sem.at[0], f_sem.at[1], peer(i))
    with jax.named_scope("final"):
        arrived(fbuf.at[pl.ds(0, N_TP - 1)], f_sem.at[1])
    total = jnp.zeros((1, 128), F32)
    for t in range(N_TP):
        total = total + fbuf[t]
    scale = jnp.broadcast_to(lax.rsqrt(total / D + EPSILON), (8, 128))
    first = jnp.where(lax.broadcasted_iota(jnp.int32, (8, W), 0) == 0, 1.0, 0.0).astype(BF16)
    hi, lo = halves(scale)
    tall = (dot(hi, first, ((0,), (0,))) + dot(lo, first, ((0,), (0,))))[:TOK]
    out[...] = (mixture * tall * fgain[...]).astype(BF16)

    seven = xbuf.at[0, 0, pl.ds(0, 7 * R)]
    sent = [(seven, ag_send.at[k]) for k in range(NEAR)] + [(seven, rs_send.at[g]) for g in range(NEAR_GROUP)]
    sent += [(q.at[:, all_near], ag_send.at[NEAR]), (q.at[:, all_near], rs_send.at[NEAR_GROUP])]
    sent += [(gbuf.at[pl.ds(0, N_TP - 1)], gsem.at[0]), (fbuf.at[pl.ds(0, N_TP - 1)], f_sem.at[0])]
    sent += [(tbuf.at[pl.ds(0, 3)], t_sem.at[0]), (mbuf, n_sem.at[0]), (sbuf.at[all_far], bulk.at[0]), (obuf.at[all_far], bulk.at[3])]
    for i, span in enumerate(parts):
        sent += [(snear.at[:, span], bulk.at[1 + i]), (tn.at[:, span], bulk.at[4 + i])]
    with jax.named_scope("drain"):
        for ref, sem in sent:
            remote(ref, ref, sem, sem, me_ep, at(yp, c)).wait_send()


def step(tokens, norm_gain, expert_ids, route_weights, gate_proj, up_proj, down_proj, final_gain):
    vmem = pltpu.VMEM
    dma = pltpu.SemaphoreType.DMA
    groups = len(GROUPS)
    return pl.pallas_call(
        kernel,
        out_shape=jax.ShapeDtypeStruct((TOK, W), BF16),
        in_specs=[pl.BlockSpec(memory_space=pltpu.HBM)] * 8,
        out_specs=pl.BlockSpec(memory_space=vmem),
        scratch_shapes=[
            vmem((NY, TOK, W), BF16),
            vmem((4, TOK), jnp.int32),
            vmem((4, TOK), F32),
            vmem((1, W), F32),
            vmem((D, W), BF16),
            vmem((D, W), BF16),
            vmem((W, D), BF16),
            vmem((N_TP, 1, W), F32),
            vmem((FAR_ROWS, W), BF16),
            vmem((NY, NEAR_ROWS, W), BF16),
            vmem((NY, 2, ROWS, W), BF16),
            vmem((NY, ROWS, W), BF16),
            vmem((NY, ROWS, W), BF16),
            vmem((NY, ROWS, W), F32),
            vmem((3, FAR_ROWS, W), BF16),
            vmem((NY, NEAR_ROWS, W), BF16),
            vmem((3, FAR_ROWS, W), BF16),
            vmem((FAR_ROWS, W), BF16),
            vmem((FAR_ROWS, W), BF16),
            vmem((NY, NEAR_ROWS, W), BF16),
            vmem((3, TOK, W), BF16),
            vmem((3, TOK, W), BF16),
            vmem((N_TP, 1, 128), F32),
            vmem((2, TOK, ROWS), BF16),
            vmem((ROWS, TOK), BF16),
            dma((8,)),
            dma((6,)),
            dma((2,)),
            dma((4,)),
            dma((2,)),
            dma((NEAR + 2,)),
            dma((NEAR + 1,)),
            dma((NEAR + 1, 4)),
            dma((groups,)),
            dma((groups, 2)),
            dma((NEAR + 2,)),
            dma((2,)),
        ],
        compiler_params=pltpu.CompilerParams(collective_id=0, has_side_effects=True, vmem_limit_bytes=50000000),
        name="moe_step",
    )(*[
        pltpu.with_memory_space_constraint(a, pltpu.HBM)
        for a in (tokens, norm_gain.reshape(1, W), expert_ids.T, route_weights.T, gate_proj, up_proj, down_proj, final_gain.reshape(1, W))
    ])


def solution(mesh):
    placed = (
        P("ep", "tp"),
        P("tp"),
        P("ep", None),
        P("ep", None),
        P("ep", None, "tp"),
        P("ep", None, "tp"),
        P("ep", "tp", None),
        P("tp"),
    )
    return jax.shard_map(step, mesh=mesh, in_specs=placed, out_specs=P("ep", "tp"), check_vma=False)
```

```python
import jax
import jax.numpy as jnp
from jax import lax
from jax.experimental import pallas as pl
from jax.experimental.pallas import tpu as pltpu
from jax.sharding import PartitionSpec as P

MESH = pl.DeviceIdType.MESH
EPSILON = 1e-05
CLAMP_LIMIT = 7.0
SIGMOID_SLOPE = 1.702
F32 = jnp.float32
BF16 = jnp.bfloat16

NZ, NX, NY = 8, 4, 4
N_EP, N_TP = NZ * NX, NY * 2
TOK, CAP, W = 64, 16, 256
D = N_TP * W
ROWS = N_EP * CAP
FAR_Z = (2, 6, 3, 5, 4)
X_OFFSETS = (0, 1, 3, 2)
NEAR_OFFSETS = (
    (1, 0), (7, 0), (1, 1), (7, 3),
    (1, 3), (7, 1), (1, 2), (7, 2),
    (0, 0), (0, 1), (0, 3), (0, 2),
)
NEAR = 5
R = ROWS // NZ
PER = NX
FAR_ROWS = NEAR * R
NEAR_ROWS = ROWS - FAR_ROWS
GROUPS = ((0, 1), (1, 2), (2, 3), (3, 4), (4, 5), (5, 8))
NEAR_GROUP = len(GROUPS) - 1
SELF = PER * NEAR + NEAR_OFFSETS.index((0, 0))
ORDER = (
    "S0 o0 o1 o2", "n0 f0 o3 o4", "n1 f1 m0 C0", "n2 f2 n3 f3",
    "C5 p0 n4 f4", "C1 P0 C2 p1", "C3 p2 C4 F0", "p3 p4 F1 F2",
    "F3 M0 F4",
)


def remote(src, dst, send_sem, recv_sem, ep, tp):
    return pltpu.make_async_remote_copy(
        src_ref=src, dst_ref=dst, send_sem=send_sem, recv_sem=recv_sem, device_id=(ep, tp), device_id_type=MESH
    )


def dot(a, b, dims=((1,), (0,))):
    return lax.dot_general(a, b, (dims, ((), ())), preferred_element_type=F32)


def kernel(
    tok_h, ngain_h, ids_h, rw_h, wg_h, wu_h, wd_h, fgain_h, out,
    tbuf, ids, rw, fgain,
    wg, wu, wd, gbuf, sbuf, snear, xbuf, ps, q, po, ts, tn, rbuf, obuf, ybuf, ynear, mbuf, nbuf, fbuf, wsel, picks,
    wsem, bulk, gsem, t_sem, n_sem, a_recv, ag_send, ag_recv, rs_send, rs_recv, y_recv, f_sem,
):
    me_ep, me_tp = lax.axis_index("ep"), lax.axis_index("tp")
    z, x = me_ep // NX, lax.rem(me_ep, NX)
    y, c = me_tp // 2, lax.rem(me_tp, 2)
    d = 1 - 2 * c
    co = 1 - c
    yp, ym, yf = lax.rem(y + d + NY, NY), lax.rem(y - d + NY, NY), lax.rem(y + 2, NY)

    def at(yy, cc):
        return yy * 2 + cc

    def offsets(p):
        return NEAR_OFFSETS[p - NEAR * PER] if p >= NEAR * PER else (FAR_Z[p // PER], X_OFFSETS[p % PER])

    def back(p):
        dz, dx = offsets(p)
        return lax.rem(z - dz + NZ, NZ) * NX + lax.rem(x - dx + NX, NX)

    def forth(p):
        dz, dx = offsets(p)
        return lax.rem(z + dz, NZ) * NX + lax.rem(x + dx, NX)

    lead = (z - 2) * ((z + NZ - 3) // NZ) * (1 - (z + 2) // NZ)

    def source(g):
        i = g - 1 + (g - 1 - lead + NZ) // NZ if g else lead
        return i + 3 * ((i - z + NZ + 1) // NZ) - 1 + (z + NZ - 1) // NZ + (z + 1) // NZ

    def chunk_of(g):
        past = lax.rem(source(g) - z + NZ, NZ) - 4
        over, under = (past + NZ - 1) // NZ, (NZ - 1 - past) // NZ
        return 4 - 2 * past * (over - under) + over

    def peer(i):
        return lax.rem(me_tp + i, N_TP)

    def hops(p):
        dz, dx = offsets(p)
        return min(dz, NZ - dz) + min(dx, NX - dx)

    far = range(NEAR * PER)
    near = [p for p in range(NEAR * PER, N_EP) if p != SELF]
    barrier = pltpu.get_barrier_semaphore()
    for p in sorted([*far, *near], key=lambda p: -hops(p)):
        pl.semaphore_signal(barrier, inc=1, device_id=(back(p), me_tp), device_id_type=MESH)
    for i in range(1, N_TP):
        pl.semaphore_signal(barrier, inc=1, device_id=(me_ep, peer(i)), device_id_type=MESH)

    small = [
        pltpu.make_async_copy(a, b, wsem.at[3 + i])
        for i, (a, b) in enumerate([(ids_h, ids), (rw_h, rw), (tok_h, tbuf.at[y]), (ngain_h, gbuf.at[me_tp]), (fgain_h, fgain)])
    ]
    loads = [
        pltpu.make_async_copy(wg_h.at[0], wg, wsem.at[0]),
        pltpu.make_async_copy(wu_h.at[0], wu, wsem.at[1]),
        pltpu.make_async_copy(wd_h.at[0], wd, wsem.at[2]),
    ]
    for load in small + loads:
        load.start()
    for load in small:
        load.wait()

    pos = lax.broadcasted_iota(jnp.int32, (N_EP, TOK), 0)
    expert = jnp.zeros_like(pos)
    for p in range(N_EP):
        expert = jnp.where(pos == p, back(p), expert)
    match = jnp.zeros((N_EP, TOK), F32)
    weight = jnp.zeros((N_EP, TOK), F32)
    for k in range(ids.shape[0]):
        hit = ids[k : k + 1, :] == expert
        match = match + jnp.where(hit, 1.0, 0.0)
        weight = weight + jnp.where(hit, rw[k : k + 1, :], 0.0)
    before = lax.broadcasted_iota(jnp.int32, (TOK, TOK), 0) < lax.broadcasted_iota(jnp.int32, (TOK, TOK), 1)
    earlier = dot(match.astype(BF16), jnp.where(before, 1.0, 0.0).astype(BF16))
    row = lax.broadcasted_iota(jnp.int32, (ROWS, N_EP), 0)
    col = lax.broadcasted_iota(jnp.int32, (ROWS, N_EP), 1)
    spread = jnp.where(row // CAP == col, 1.0, 0.0).astype(BF16)
    slot = lax.rem(lax.broadcasted_iota(jnp.int32, (ROWS, TOK), 0), CAP).astype(F32)
    taken = (dot(spread, earlier.astype(BF16)) == slot) & (dot(spread, match.astype(BF16)) > 0.5)
    picks[...] = jnp.where(taken, 1.0, 0.0).astype(BF16)
    sbuf[...] = dot(picks[0:FAR_ROWS], tbuf[y]).astype(BF16)
    with jax.named_scope("barrier"):
        pl.semaphore_wait(barrier, N_EP - 1 + N_TP - 1)

    def block(p):
        return pl.ds(p * CAP, CAP)

    def near_block(p):
        return pl.ds(p * CAP - FAR_ROWS, CAP)

    def chunk(k):
        return pl.ds(k * R, R)

    def group(g):
        lo, hi = GROUPS[g]
        return pl.ds(lo * R, (hi - lo) * R)

    all_far = pl.ds(0, FAR_ROWS)
    all_near = pl.ds(FAR_ROWS, NEAR_ROWS)
    own = SELF * CAP - FAR_ROWS
    parts = (pl.ds(0, own), pl.ds(own + CAP, NEAR_ROWS - own - CAP))
    def send(src, dst, send_sem, recv_sem, tp):
        remote(src, dst, send_sem, recv_sem, me_ep, tp).start()

    def arrived(ref, sem):
        remote(ref, ref, bulk.at[0], sem, me_ep, at(yp, c)).wait_recv()

    for i, yy in enumerate((yf, yp, ym)):
        send(tbuf.at[y], tbuf.at[y], t_sem.at[0], t_sem.at[1 + i], at(yy, c))
    def far_dispatch(positions):
        for p in positions:
            remote(sbuf.at[block(p)], xbuf.at[y, c, block(p)], bulk.at[0], a_recv.at[p // PER], back(p), me_tp).start()

    far_dispatch(far[: 2 * PER])

    @pl.when(c == 0)
    def _():
        far_dispatch(far[2 * PER :])

    for i in range(1, N_TP):
        send(gbuf.at[me_tp], gbuf.at[me_tp], gsem.at[0], gsem.at[1], peer(i))

    w_hi = weight.astype(BF16)
    w_lo = (weight - w_hi.astype(F32)).astype(BF16)
    chosen = jnp.where(taken, dot(spread, w_hi) + dot(spread, w_lo), 0.0).T
    c_hi = chosen.astype(BF16)
    wsel[0] = c_hi
    wsel[1] = (chosen - c_hi.astype(F32)).astype(BF16)

    def near_dispatch(_):
        arrived(tbuf.at[ym], t_sem.at[2])

        @pl.when(c == 1)
        def _():
            far_dispatch(far[2 * PER :])

        arrived(tbuf.at[yp], t_sem.at[3])
        arrived(tbuf.at[yf], t_sem.at[1])
        for yy in range(NY):
            rows = dot(picks[FAR_ROWS:ROWS], tbuf[yy]).astype(BF16)
            snear[yy] = rows
            xbuf[yy, c, SELF * CAP : (SELF + 1) * CAP] = rows[own : own + CAP]
        for p in near:
            i = int(p > SELF)
            remote(snear.at[:, near_block(p)], xbuf.at[:, c, block(p)], bulk.at[0], a_recv.at[NEAR + i], back(p), me_tp).start()

    def near_share(_):
        for i, span in enumerate(parts):
            ref = xbuf.at[:, c, pl.ds(FAR_ROWS + span.start, span.size)]
            arrived(ref, a_recv.at[NEAR + i])
        ref = xbuf.at[:, c, all_near]
        send(ref, ref, ag_send.at[0], ag_recv.at[NEAR, 3], at(y, co))

    def gather_own(k):
        ref = xbuf.at[y, c, chunk(k)]
        arrived(ref, a_recv.at[k])
        for i, tp in ((2, at(yf, c)), (0, at(yp, c)), (1, at(ym, c)), (3, at(y, co))):
            send(ref, ref, ag_send.at[0], ag_recv.at[k, i], tp)

    def gather_near(k):
        ref = xbuf.at[ym, c, chunk(k)]
        arrived(ref, ag_recv.at[k, 0])
        send(ref, ref, ag_send.at[0], ag_recv.at[k, 3], at(y, co))
        ref = xbuf.at[yp, c, chunk(k)]
        arrived(ref, ag_recv.at[k, 1])
        send(ref, ref, ag_send.at[0], ag_recv.at[k, 3], at(y, co))

    def gather_far(k):
        ref = xbuf.at[yf, c, chunk(k)]
        arrived(ref, ag_recv.at[k, 2])
        send(ref, ref, ag_send.at[0], ag_recv.at[k, 3], at(y, co))

    def compute(g):
        if loads:
            arrived(gbuf.at[pl.ds(0, N_TP - 1)], gsem.at[1])
        while loads:
            loads.pop().wait()
        if g == NEAR_GROUP:
            arrived(xbuf.at[:, co, all_near], ag_recv.at[NEAR, 3])
            held = all_near
        else:
            held = pl.ds(pl.multiple_of(chunk_of(g) * R, R), R)
            arrived(xbuf.at[:, co, held], ag_recv.at[chunk_of(g), 3])
        rows = group(g)
        squares = jnp.zeros((rows.size, W), F32)
        for t in range(N_TP):
            part = xbuf[t // 2, t % 2, held].astype(F32)
            squares = squares + part * part
        scale = lax.rsqrt(jnp.sum(squares, axis=1, keepdims=True) / D + EPSILON)
        gate = jnp.zeros((rows.size, W), F32)
        up = jnp.zeros((rows.size, W), F32)
        for t in range(N_TP):
            part = xbuf[t // 2, t % 2, held].astype(F32)
            normed = (part * scale * gbuf[t]).astype(BF16)
            gate = gate + dot(normed, wg[t * W : (t + 1) * W, :])
            up = up + dot(normed, wu[t * W : (t + 1) * W, :])
        gate = jnp.minimum(gate, CLAMP_LIMIT)
        up = jnp.clip(up, -CLAMP_LIMIT, CLAMP_LIMIT)
        act = ((up + 1.0) * gate * jax.nn.sigmoid(SIGMOID_SLOPE * gate)).astype(BF16)
        for yy in range(NY):
            ps[yy, rows] = dot(act, wd[:, pl.ds(pl.multiple_of(at(yy, co) * W, W), W)]).astype(BF16)
        send(ps.at[:, rows], q.at[:, rows], rs_send.at[0], rs_recv.at[g, 0], at(y, co))
        for yy in range(NY):
            po[yy, rows] = dot(act, wd[:, pl.ds(pl.multiple_of(at(yy, c) * W, W), W)])

    def pair(yy, rows):
        return po[yy, rows] + q[yy, rows].astype(F32)

    def pair_sum(g):
        rows = group(g)
        arrived(q.at[:, rows], rs_recv.at[g, 0])
        for i, yy in enumerate((yf, ym, yp)):
            ts[i, rows] = pair(yy, rows).astype(BF16)
            send(ts.at[i, rows], rbuf.at[i, rows], rs_send.at[0], rs_recv.at[g, 1], at(yy, c))

    def finish(g):
        rows = group(g)
        total = pair(y, rows)
        arrived(rbuf.at[:, rows], rs_recv.at[g, 1])
        for i in range(3):
            total = total + rbuf[i, rows].astype(F32)
        obuf[rows] = total.astype(BF16)
        for i, dx in enumerate(X_OFFSETS):
            place = pl.ds(pl.multiple_of(chunk_of(g) * R + i * CAP, CAP), CAP)
            device = source(g) * NX + lax.rem(x + dx, NX)
            remote(obuf.at[block(g * PER + i)], ybuf.at[place], bulk.at[0], y_recv.at[chunk_of(g)], device, me_tp).start()

    def near_return(_):
        arrived(q.at[:, all_near], rs_recv.at[NEAR_GROUP, 0])
        for yy in range(NY):
            rows = pair(yy, all_near).astype(BF16)
            tn[yy] = rows
            ynear[yy, own : own + CAP] = rows[own : own + CAP]
        for p in near:
            i = int(p > SELF)
            remote(tn.at[:, near_block(p)], ynear.at[:, near_block(p)], bulk.at[0], y_recv.at[NEAR + i], forth(p), me_tp).start()

    def mixed(columns, values):
        return dot(wsel[0, :, columns], values) + dot(wsel[1, :, columns], values)

    mixture = []

    def near_mix(_):
        for i, span in enumerate(parts):
            arrived(ynear.at[:, span], y_recv.at[NEAR + i])
        for i, yy in enumerate((yf, yp, ym)):
            mbuf[i] = mixed(slice(FAR_ROWS, ROWS), ynear[yy]).astype(BF16)
            send(mbuf.at[i], nbuf.at[i], n_sem.at[0], n_sem.at[1], at(yy, c))
        mixture.append(mixed(slice(FAR_ROWS, ROWS), ynear[y]))

    stages = dict(
        S=near_dispatch, m=near_share, o=gather_own, n=gather_near, f=gather_far, C=compute, p=pair_sum, F=finish,
        P=near_return, M=near_mix,
    )
    for item in " ".join(ORDER).split():
        with jax.named_scope(item):
            stages[item[0]](int(item[1:]))

    (mixture,) = mixture
    for k in range(NEAR):
        with jax.named_scope(f"return{k}"):
            arrived(ybuf.at[chunk(k)], y_recv.at[k])
        mixture = mixture + mixed(slice(k * R, (k + 1) * R), ybuf[chunk(k)])
    with jax.named_scope("near_sum"):
        arrived(nbuf, n_sem.at[1])
    for i in range(3):
        mixture = mixture + nbuf[i].astype(F32)

    def halves(a):
        hi = a.astype(BF16)
        return hi, (a - hi.astype(F32)).astype(BF16)

    ones = jnp.ones((8, W), BF16)
    hi, lo = halves(mixture * mixture)
    sums = dot(ones, hi, ((1,), (1,))) + dot(ones, lo, ((1,), (1,)))
    fbuf[me_tp] = jnp.concatenate([sums, jnp.zeros((8, 128 - TOK), F32)], axis=1)[0:1]
    for i in (4, 3, 5, 2, 6, 7, 1):
        send(fbuf.at[me_tp], fbuf.at[me_tp], f_sem.at[0], f_sem.at[1], peer(i))
    with jax.named_scope("final"):
        arrived(fbuf.at[pl.ds(0, N_TP - 1)], f_sem.at[1])
    total = jnp.zeros((1, 128), F32)
    for t in range(N_TP):
        total = total + fbuf[t]
    scale = jnp.broadcast_to(lax.rsqrt(total / D + EPSILON), (8, 128))
    first = jnp.where(lax.broadcasted_iota(jnp.int32, (8, W), 0) == 0, 1.0, 0.0).astype(BF16)
    hi, lo = halves(scale)
    tall = (dot(hi, first, ((0,), (0,))) + dot(lo, first, ((0,), (0,))))[:TOK]
    out[...] = (mixture * tall * fgain[...]).astype(BF16)

    gathered = po.at[:, pl.ds(0, (7 * FAR_ROWS + NY * NEAR_ROWS) // (2 * NY))]
    sent = [(gathered, ag_send.at[0]), (gathered, rs_send.at[0]), (q, bulk.at[0]), (tbuf.at[pl.ds(0, 3)], t_sem.at[0])]
    sent += [(gbuf.at[pl.ds(0, N_TP - 1)], gsem.at[0]), (fbuf.at[pl.ds(0, N_TP - 1)], f_sem.at[0]), (mbuf, n_sem.at[0])]
    with jax.named_scope("drain"):
        for ref, sem in sent:
            remote(ref, ref, sem, sem, me_ep, at(yp, c)).wait_send()


def step(tokens, norm_gain, expert_ids, route_weights, gate_proj, up_proj, down_proj, final_gain):
    vmem = pltpu.VMEM
    dma = pltpu.SemaphoreType.DMA
    groups = len(GROUPS)
    return pl.pallas_call(
        kernel,
        out_shape=jax.ShapeDtypeStruct((TOK, W), BF16),
        in_specs=[pl.BlockSpec(memory_space=pltpu.HBM)] * 8,
        out_specs=pl.BlockSpec(memory_space=vmem),
        scratch_shapes=[
            vmem((NY, TOK, W), BF16),
            vmem((4, TOK), jnp.int32),
            vmem((4, TOK), F32),
            vmem((1, W), F32),
            vmem((D, W), BF16),
            vmem((D, W), BF16),
            vmem((W, D), BF16),
            vmem((N_TP, 1, W), F32),
            vmem((FAR_ROWS, W), BF16),
            vmem((NY, NEAR_ROWS, W), BF16),
            vmem((NY, 2, ROWS, W), BF16),
            vmem((NY, ROWS, W), BF16),
            vmem((NY, ROWS, W), BF16),
            vmem((NY, ROWS, W), F32),
            vmem((3, FAR_ROWS, W), BF16),
            vmem((NY, NEAR_ROWS, W), BF16),
            vmem((3, FAR_ROWS, W), BF16),
            vmem((FAR_ROWS, W), BF16),
            vmem((FAR_ROWS, W), BF16),
            vmem((NY, NEAR_ROWS, W), BF16),
            vmem((3, TOK, W), BF16),
            vmem((3, TOK, W), BF16),
            vmem((N_TP, 1, 128), F32),
            vmem((2, TOK, ROWS), BF16),
            vmem((ROWS, TOK), BF16),
            dma((8,)),
            dma((1,)),
            dma((2,)),
            dma((4,)),
            dma((2,)),
            dma((NEAR + 2,)),
            dma((1,)),
            dma((NEAR + 1, 4)),
            dma((1,)),
            dma((groups, 2)),
            dma((NEAR + 2,)),
            dma((2,)),
        ],
        compiler_params=pltpu.CompilerParams(collective_id=0, has_side_effects=True, vmem_limit_bytes=50000000),
        name="moe_step",
    )(*[
        pltpu.with_memory_space_constraint(a, pltpu.HBM)
        for a in (tokens, norm_gain.reshape(1, W), expert_ids.T, route_weights.T, gate_proj, up_proj, down_proj, final_gain.reshape(1, W))
    ])


def solution(mesh):
    placed = (
        P("ep", "tp"),
        P("tp"),
        P("ep", None),
        P("ep", None),
        P("ep", None, "tp"),
        P("ep", None, "tp"),
        P("ep", "tp", None),
        P("tp"),
    )
    return jax.shard_map(step, mesh=mesh, in_specs=placed, out_specs=P("ep", "tp"), check_vma=False)
```

```python
import jax
import jax.numpy as jnp
from jax import lax
from jax.experimental import pallas as pl
from jax.experimental.pallas import tpu as pltpu
from jax.sharding import PartitionSpec as P

MESH = pl.DeviceIdType.MESH
EPSILON = 1e-05
CLAMP_LIMIT = 7.0
SIGMOID_SLOPE = 1.702
F32 = jnp.float32
BF16 = jnp.bfloat16

NZ, NX, NY = 8, 4, 4
N_EP, N_TP = NZ * NX, NY * 2
TOK, CAP, W = 64, 16, 256
D = N_TP * W
ROWS = N_EP * CAP
FAR_Z = (2, 6, 3, 5, 4)
X_OFFSETS = (0, 1, 3, 2)
NEAR_OFFSETS = (
    (1, 0), (7, 0), (1, 1), (7, 3),
    (1, 3), (7, 1), (1, 2), (7, 2),
    (0, 0), (0, 1), (0, 3), (0, 2),
)
NEAR = 5
R = ROWS // NZ
PER = NX
FAR_ROWS = NEAR * R
NEAR_ROWS = ROWS - FAR_ROWS
GROUPS = ((0, 1), (1, 2), (2, 3), (3, 4), (4, 5), (5, 8))
NEAR_GROUP = len(GROUPS) - 1
SELF = PER * NEAR + NEAR_OFFSETS.index((0, 0))
ORDER = (
    "S0 o0 o1 o2", "n0 f0 o3 o4", "n1 f1 m0 C0", "n2 f2 n3 f3",
    "C5 p0 n4 f4", "C1 P0 C2 p1", "C3 p2 C4 F0", "p3 p4 F1 F2",
    "F3 M0 F4",
)


def remote(src, dst, send_sem, recv_sem, ep, tp):
    return pltpu.make_async_remote_copy(
        src_ref=src, dst_ref=dst, send_sem=send_sem, recv_sem=recv_sem, device_id=(ep, tp), device_id_type=MESH
    )


def dot(a, b, dims=((1,), (0,))):
    return lax.dot_general(a, b, (dims, ((), ())), preferred_element_type=F32)


def kernel(
    tok_h, ngain_h, ids_h, rw_h, wg_h, wu_h, wd_h, fgain_h, out,
    tbuf, ids, rw, fgain,
    wg, wu, wd, gbuf, sbuf, snear, xbuf, ps, q, po, ts, tn, rbuf, obuf, ybuf, ynear, mbuf, nbuf, fbuf, wsel, picks,
    wsem, bulk, gsem, t_sem, n_sem, a_recv, ag_send, ag_recv, rs_send, rs_recv, y_recv, f_sem,
):
    me_ep, me_tp = lax.axis_index("ep"), lax.axis_index("tp")
    z, x = me_ep // NX, lax.rem(me_ep, NX)
    y, c = me_tp // 2, lax.rem(me_tp, 2)
    d = 1 - 2 * c
    co = 1 - c
    yp, ym, yf = lax.rem(y + d + NY, NY), lax.rem(y - d + NY, NY), lax.rem(y + 2, NY)

    def at(yy, cc):
        return yy * 2 + cc

    def offsets(p):
        return NEAR_OFFSETS[p - NEAR * PER] if p >= NEAR * PER else (FAR_Z[p // PER], X_OFFSETS[p % PER])

    def back(p):
        dz, dx = offsets(p)
        return lax.rem(z - dz + NZ, NZ) * NX + lax.rem(x - dx + NX, NX)

    def forth(p):
        dz, dx = offsets(p)
        return lax.rem(z + dz, NZ) * NX + lax.rem(x + dx, NX)

    lead = (z - 2) * ((z + NZ - 3) // NZ) * (1 - (z + 2) // NZ)

    def source(g):
        i = g - 1 + (g - 1 - lead + NZ) // NZ if g else lead
        return i + 3 * ((i - z + NZ + 1) // NZ) - 1 + (z + NZ - 1) // NZ + (z + 1) // NZ

    def chunk_of(g):
        past = lax.rem(source(g) - z + NZ, NZ) - 4
        over, under = (past + NZ - 1) // NZ, (NZ - 1 - past) // NZ
        return 4 - 2 * past * (over - under) + over

    def peer(i):
        return lax.rem(me_tp + i, N_TP)

    def hops(p):
        dz, dx = offsets(p)
        return min(dz, NZ - dz) + min(dx, NX - dx)

    far = range(NEAR * PER)
    near = [p for p in range(NEAR * PER, N_EP) if p != SELF]
    barrier = pltpu.get_barrier_semaphore()
    for p in sorted([*far, *near], key=lambda p: -hops(p)):
        pl.semaphore_signal(barrier, inc=1, device_id=(back(p), me_tp), device_id_type=MESH)
    for i in range(1, N_TP):
        pl.semaphore_signal(barrier, inc=1, device_id=(me_ep, peer(i)), device_id_type=MESH)

    small = [
        pltpu.make_async_copy(a, b, wsem.at[3 + i])
        for i, (a, b) in enumerate([(ids_h, ids), (rw_h, rw), (tok_h, tbuf.at[y]), (ngain_h, gbuf.at[me_tp]), (fgain_h, fgain)])
    ]
    loads = [
        pltpu.make_async_copy(wg_h.at[0], wg, wsem.at[0]),
        pltpu.make_async_copy(wu_h.at[0], wu, wsem.at[1]),
        pltpu.make_async_copy(wd_h.at[0], wd, wsem.at[2]),
    ]
    for load in small + loads:
        load.start()
    for load in small:
        load.wait()

    pos = lax.broadcasted_iota(jnp.int32, (N_EP, TOK), 0)
    expert = jnp.zeros_like(pos)
    for p in range(N_EP):
        expert = jnp.where(pos == p, back(p), expert)
    match = jnp.zeros((N_EP, TOK), F32)
    weight = jnp.zeros((N_EP, TOK), F32)
    for k in range(ids.shape[0]):
        hit = ids[k : k + 1, :] == expert
        match = match + jnp.where(hit, 1.0, 0.0)
        weight = weight + jnp.where(hit, rw[k : k + 1, :], 0.0)
    before = lax.broadcasted_iota(jnp.int32, (TOK, TOK), 0) < lax.broadcasted_iota(jnp.int32, (TOK, TOK), 1)
    earlier = dot(match.astype(BF16), jnp.where(before, 1.0, 0.0).astype(BF16))
    row = lax.broadcasted_iota(jnp.int32, (ROWS, N_EP), 0)
    col = lax.broadcasted_iota(jnp.int32, (ROWS, N_EP), 1)
    spread = jnp.where(row // CAP == col, 1.0, 0.0).astype(BF16)
    slot = lax.rem(lax.broadcasted_iota(jnp.int32, (ROWS, TOK), 0), CAP).astype(F32)
    taken = (dot(spread, earlier.astype(BF16)) == slot) & (dot(spread, match.astype(BF16)) > 0.5)
    picks[...] = jnp.where(taken, 1.0, 0.0).astype(BF16)
    sbuf[...] = dot(picks[0:FAR_ROWS], tbuf[y]).astype(BF16)
    with jax.named_scope("barrier"):
        pl.semaphore_wait(barrier, N_EP - 1 + N_TP - 1)

    def block(p):
        return pl.ds(p * CAP, CAP)

    def near_block(p):
        return pl.ds(p * CAP - FAR_ROWS, CAP)

    def chunk(k):
        return pl.ds(k * R, R)

    def group(g):
        lo, hi = GROUPS[g]
        return pl.ds(lo * R, (hi - lo) * R)

    all_far = pl.ds(0, FAR_ROWS)
    all_near = pl.ds(FAR_ROWS, NEAR_ROWS)
    own = SELF * CAP - FAR_ROWS
    parts = (pl.ds(0, own), pl.ds(own + CAP, NEAR_ROWS - own - CAP))
    def send(src, dst, send_sem, recv_sem, tp):
        remote(src, dst, send_sem, recv_sem, me_ep, tp).start()

    def arrived(ref, sem):
        remote(ref, ref, bulk.at[0], sem, me_ep, at(yp, c)).wait_recv()

    for i, yy in enumerate((yf, yp, ym)):
        send(tbuf.at[y], tbuf.at[y], t_sem.at[0], t_sem.at[1 + i], at(yy, c))
    def far_dispatch(positions):
        for p in positions:
            remote(sbuf.at[block(p)], xbuf.at[y, c, block(p)], bulk.at[0], a_recv.at[p // PER], back(p), me_tp).start()

    far_dispatch(far[: 2 * PER])

    @pl.when(c == 0)
    def _():
        far_dispatch(far[2 * PER :])

    for i in range(1, N_TP):
        send(gbuf.at[me_tp], gbuf.at[me_tp], gsem.at[0], gsem.at[1], peer(i))

    w_hi = weight.astype(BF16)
    w_lo = (weight - w_hi.astype(F32)).astype(BF16)
    chosen = jnp.where(taken, dot(spread, w_hi) + dot(spread, w_lo), 0.0).T
    c_hi = chosen.astype(BF16)
    wsel[0] = c_hi
    wsel[1] = (chosen - c_hi.astype(F32)).astype(BF16)

    def near_dispatch(_):
        arrived(tbuf.at[ym], t_sem.at[2])

        @pl.when(c == 1)
        def _():
            far_dispatch(far[2 * PER :])

        arrived(tbuf.at[yp], t_sem.at[3])
        arrived(tbuf.at[yf], t_sem.at[1])
        for yy in range(NY):
            rows = dot(picks[FAR_ROWS:ROWS], tbuf[yy]).astype(BF16)
            snear[yy] = rows
            xbuf[yy, c, SELF * CAP : (SELF + 1) * CAP] = rows[own : own + CAP]
        for p in near:
            i = int(p > SELF)
            remote(snear.at[:, near_block(p)], xbuf.at[:, c, block(p)], bulk.at[0], a_recv.at[NEAR + i], back(p), me_tp).start()

    def near_share(_):
        for i, span in enumerate(parts):
            ref = xbuf.at[:, c, pl.ds(FAR_ROWS + span.start, span.size)]
            arrived(ref, a_recv.at[NEAR + i])
        ref = xbuf.at[:, c, all_near]
        send(ref, ref, ag_send.at[0], ag_recv.at[NEAR, 3], at(y, co))

    def gather_own(k):
        ref = xbuf.at[y, c, chunk(k)]
        arrived(ref, a_recv.at[k])
        for i, tp in ((2, at(yf, c)), (0, at(yp, c)), (1, at(ym, c)), (3, at(y, co))):
            send(ref, ref, ag_send.at[0], ag_recv.at[k, i], tp)

    def gather_near(k):
        ref = xbuf.at[ym, c, chunk(k)]
        arrived(ref, ag_recv.at[k, 0])
        send(ref, ref, ag_send.at[0], ag_recv.at[k, 3], at(y, co))
        ref = xbuf.at[yp, c, chunk(k)]
        arrived(ref, ag_recv.at[k, 1])
        send(ref, ref, ag_send.at[0], ag_recv.at[k, 3], at(y, co))

    def gather_far(k):
        ref = xbuf.at[yf, c, chunk(k)]
        arrived(ref, ag_recv.at[k, 2])
        send(ref, ref, ag_send.at[0], ag_recv.at[k, 3], at(y, co))

    def compute(g):
        if loads:
            arrived(gbuf.at[pl.ds(0, N_TP - 1)], gsem.at[1])
        while loads:
            loads.pop().wait()
        if g == NEAR_GROUP:
            arrived(xbuf.at[:, co, all_near], ag_recv.at[NEAR, 3])
            held = all_near
        else:
            held = pl.ds(pl.multiple_of(chunk_of(g) * R, R), R)
            arrived(xbuf.at[:, co, held], ag_recv.at[chunk_of(g), 3])
        rows = group(g)
        squares = jnp.zeros((rows.size, W), F32)
        for t in range(N_TP):
            part = xbuf[t // 2, t % 2, held].astype(F32)
            squares = squares + part * part
        scale = lax.rsqrt(jnp.sum(squares, axis=1, keepdims=True) / D + EPSILON)
        gate = jnp.zeros((rows.size, W), F32)
        up = jnp.zeros((rows.size, W), F32)
        for t in range(N_TP):
            part = xbuf[t // 2, t % 2, held].astype(F32)
            normed = (part * scale * gbuf[t]).astype(BF16)
            gate = gate + dot(normed, wg[t * W : (t + 1) * W, :])
            up = up + dot(normed, wu[t * W : (t + 1) * W, :])
        gate = jnp.minimum(gate, CLAMP_LIMIT)
        up = jnp.clip(up, -CLAMP_LIMIT, CLAMP_LIMIT)
        act = ((up + 1.0) * gate * jax.nn.sigmoid(SIGMOID_SLOPE * gate)).astype(BF16)
        for yy in range(NY):
            ps[yy, rows] = dot(act, wd[:, pl.ds(pl.multiple_of(at(yy, co) * W, W), W)]).astype(BF16)
        send(ps.at[:, rows], q.at[:, rows], rs_send.at[0], rs_recv.at[g, 0], at(y, co))
        for yy in range(NY):
            po[yy, rows] = dot(act, wd[:, pl.ds(pl.multiple_of(at(yy, c) * W, W), W)])

    def pair(yy, rows):
        return po[yy, rows] + q[yy, rows].astype(F32)

    def pair_sum(g):
        rows = group(g)
        arrived(q.at[:, rows], rs_recv.at[g, 0])
        for i, yy in enumerate((yf, ym, yp)):
            ts[i, rows] = pair(yy, rows).astype(BF16)
            send(ts.at[i, rows], rbuf.at[i, rows], rs_send.at[0], rs_recv.at[g, 1], at(yy, c))

    def finish(g):
        rows = group(g)
        total = pair(y, rows)
        arrived(rbuf.at[:, rows], rs_recv.at[g, 1])
        for i in range(3):
            total = total + rbuf[i, rows].astype(F32)
        obuf[rows] = total.astype(BF16)
        for i, dx in enumerate(X_OFFSETS):
            place = pl.ds(pl.multiple_of(chunk_of(g) * R + i * CAP, CAP), CAP)
            device = source(g) * NX + lax.rem(x + dx, NX)
            remote(obuf.at[block(g * PER + i)], ybuf.at[place], bulk.at[0], y_recv.at[chunk_of(g)], device, me_tp).start()

    def near_return(_):
        arrived(q.at[:, all_near], rs_recv.at[NEAR_GROUP, 0])
        for yy in range(NY):
            rows = pair(yy, all_near).astype(BF16)
            tn[yy] = rows
            ynear[yy, own : own + CAP] = rows[own : own + CAP]
        for p in near:
            i = int(p > SELF)
            remote(tn.at[:, near_block(p)], ynear.at[:, near_block(p)], bulk.at[0], y_recv.at[NEAR + i], forth(p), me_tp).start()

    def mixed(columns, values):
        return dot(wsel[0, :, columns], values) + dot(wsel[1, :, columns], values)

    mixture = []

    def near_mix(_):
        for i, span in enumerate(parts):
            arrived(ynear.at[:, span], y_recv.at[NEAR + i])
        for i, yy in enumerate((yf, yp, ym)):
            mbuf[i] = mixed(slice(FAR_ROWS, ROWS), ynear[yy]).astype(BF16)
            send(mbuf.at[i], nbuf.at[i], n_sem.at[0], n_sem.at[1], at(yy, c))
        mixture.append(mixed(slice(FAR_ROWS, ROWS), ynear[y]))

    stages = dict(
        S=near_dispatch, m=near_share, o=gather_own, n=gather_near, f=gather_far, C=compute, p=pair_sum, F=finish,
        P=near_return, M=near_mix,
    )
    for item in " ".join(ORDER).split():
        with jax.named_scope(item):
            stages[item[0]](int(item[1:]))

    (mixture,) = mixture
    for k in range(NEAR):
        with jax.named_scope(f"return{k}"):
            arrived(ybuf.at[chunk(k)], y_recv.at[k])
        mixture = mixture + mixed(slice(k * R, (k + 1) * R), ybuf[chunk(k)])
    with jax.named_scope("near_sum"):
        arrived(nbuf, n_sem.at[1])
    for i in range(3):
        mixture = mixture + nbuf[i].astype(F32)

    def halves(a):
        hi = a.astype(BF16)
        return hi, (a - hi.astype(F32)).astype(BF16)

    sums = jnp.sum(mixture * mixture, axis=1, keepdims=True)
    sums = jnp.broadcast_to(jnp.concatenate([sums, jnp.zeros((128 - TOK, 1), F32)], axis=0), (128, 128))
    fbuf[me_tp] = sums.T[0:1]
    for i in (4, 3, 5, 2, 6, 7, 1):
        send(fbuf.at[me_tp], fbuf.at[me_tp], f_sem.at[0], f_sem.at[1], peer(i))
    with jax.named_scope("final"):
        arrived(fbuf.at[pl.ds(0, N_TP - 1)], f_sem.at[1])
    total = jnp.zeros((1, 128), F32)
    for t in range(N_TP):
        total = total + fbuf[t]
    scale = jnp.broadcast_to(lax.rsqrt(total / D + EPSILON), (8, 128))
    first = jnp.where(lax.broadcasted_iota(jnp.int32, (8, W), 0) == 0, 1.0, 0.0).astype(BF16)
    hi, lo = halves(scale)
    tall = (dot(hi, first, ((0,), (0,))) + dot(lo, first, ((0,), (0,))))[:TOK]
    out[...] = (mixture * tall * fgain[...]).astype(BF16)

    gathered = po.at[:, pl.ds(0, (7 * FAR_ROWS + NY * NEAR_ROWS) // (2 * NY))]
    sent = [(gathered, ag_send.at[0]), (gathered, rs_send.at[0]), (q, bulk.at[0]), (tbuf.at[pl.ds(0, 3)], t_sem.at[0])]
    sent += [(gbuf.at[pl.ds(0, N_TP - 1)], gsem.at[0]), (fbuf.at[pl.ds(0, N_TP - 1)], f_sem.at[0]), (mbuf, n_sem.at[0])]
    with jax.named_scope("drain"):
        for ref, sem in sent:
            remote(ref, ref, sem, sem, me_ep, at(yp, c)).wait_send()


def step(tokens, norm_gain, expert_ids, route_weights, gate_proj, up_proj, down_proj, final_gain):
    vmem = pltpu.VMEM
    dma = pltpu.SemaphoreType.DMA
    groups = len(GROUPS)
    return pl.pallas_call(
        kernel,
        out_shape=jax.ShapeDtypeStruct((TOK, W), BF16),
        in_specs=[pl.BlockSpec(memory_space=pltpu.HBM)] * 8,
        out_specs=pl.BlockSpec(memory_space=vmem),
        scratch_shapes=[
            vmem((NY, TOK, W), BF16),
            vmem((4, TOK), jnp.int32),
            vmem((4, TOK), F32),
            vmem((1, W), F32),
            vmem((D, W), BF16),
            vmem((D, W), BF16),
            vmem((W, D), BF16),
            vmem((N_TP, 1, W), F32),
            vmem((FAR_ROWS, W), BF16),
            vmem((NY, NEAR_ROWS, W), BF16),
            vmem((NY, 2, ROWS, W), BF16),
            vmem((NY, ROWS, W), BF16),
            vmem((NY, ROWS, W), BF16),
            vmem((NY, ROWS, W), F32),
            vmem((3, FAR_ROWS, W), BF16),
            vmem((NY, NEAR_ROWS, W), BF16),
            vmem((3, FAR_ROWS, W), BF16),
            vmem((FAR_ROWS, W), BF16),
            vmem((FAR_ROWS, W), BF16),
            vmem((NY, NEAR_ROWS, W), BF16),
            vmem((3, TOK, W), BF16),
            vmem((3, TOK, W), BF16),
            vmem((N_TP, 1, 128), F32),
            vmem((2, TOK, ROWS), BF16),
            vmem((ROWS, TOK), BF16),
            dma((8,)),
            dma((1,)),
            dma((2,)),
            dma((4,)),
            dma((2,)),
            dma((NEAR + 2,)),
            dma((1,)),
            dma((NEAR + 1, 4)),
            dma((1,)),
            dma((groups, 2)),
            dma((NEAR + 2,)),
            dma((2,)),
        ],
        compiler_params=pltpu.CompilerParams(collective_id=0, has_side_effects=True, vmem_limit_bytes=50000000),
        name="moe_step",
    )(*[
        pltpu.with_memory_space_constraint(a, pltpu.HBM)
        for a in (tokens, norm_gain.reshape(1, W), expert_ids.T, route_weights.T, gate_proj, up_proj, down_proj, final_gain.reshape(1, W))
    ])


def solution(mesh):
    placed = (
        P("ep", "tp"),
        P("tp"),
        P("ep", None),
        P("ep", None),
        P("ep", None, "tp"),
        P("ep", None, "tp"),
        P("ep", "tp", None),
        P("tp"),
    )
    return jax.shard_map(step, mesh=mesh, in_specs=placed, out_specs=P("ep", "tp"), check_vma=False)
```
